256 devices in a mesh: grp: 2 (over y), ep: 32 (over z, core), tp: 4 (over x).
Axes of the slice: x: 4, y: 2, z: 16, core: 2. Of those that a mesh axis runs over, the one named last changes fastest.
The devices are a block of a 4x16x16 slice.
Arguments:
- queries: bfloat16 [16384, 2048], P(('grp', 'ep'), 'tp'), parts along dimension 0, may hold values from -8 to 8
- key_rows: bfloat16 [16384, 2048], P(('grp', 'ep'), 'tp'), parts along dimension 0, may hold values from -8 to 8
- value_rows: bfloat16 [16384, 2048], P(('grp', 'ep'), 'tp'), parts along dimension 0, may hold values from -6 to 6
- mix_lambda: float32 [32], P('tp'), may hold values from 0.3 to 0.8
- head_gain: float32 [64], replicated, may hold values from 0.1 to 1.9
- out_weight: bfloat16 [2048, 2048], P('tp'), may hold values from -0.125 to 0.125
- expert_in: bfloat16 [16384, 2048], P(('grp', 'ep', 'tp')), parts along dimension 0, may hold values from -6 to 6
- expert_gain: float32 [2048], replicated, may hold values from 0.1 to 1.9
- routes: int32 [16384, 2], P(('grp', 'ep', 'tp')), parts along dimension 0, may hold values from 0 to 31, all different within a row; in each aligned block of 64 rows (0 to 63, 64 to 127, ...) at most 5 rows name the same one
- route_logits: float32 [16384, 2], P(('grp', 'ep', 'tp')), parts along dimension 0, may hold values from -6 to 6
- gate_weight: bfloat16 [32, 2048, 2048], P('ep', None, 'tp'), may hold values from -1 to 1
- up_weight: bfloat16 [32, 2048, 2048], P('ep', None, 'tp'), may hold values from -1 to 1
- down_weight: bfloat16 [32, 2048, 2048], P('ep', 'tp'), may hold values from -0.125 to 0.125
Outputs:
- mixer_out: bfloat16 [16384, 2048], P(('grp', 'ep', 'tp')), parts along dimension 0
- expert_out: bfloat16 [16384, 2048], P(('grp', 'ep', 'tp')), parts along dimension 0
The draws below stay inside these ranges and needn't reach their ends.
There are 2 independent parts, one for each index of `grp`. The reference program is written for one: setup_inputs(seed, part) draws one part's arguments, and reference() takes and returns one part's arrays. A program takes and returns all parts, laid end to end along the dimension named above; an argument that names none is the same for every part. Nothing has to cross between parts.
Inputs may be any that keep to these rules, and one draw needn't show every extreme that they name: `routes`: each row names 2 different experts; in each aligned block of 64 rows (the rows of one device) no expert is named by more than 5 rows, a bound that some block reaches.
All inputs are finite; a program needn't handle non-finite values.
Results may differ from the reference program's by a relative error of at most 0.014.
Values may be sent and summed in bfloat16 or wider, within the bound.
A program may use at most 128 MiB of HBM per device.

```python
import math
import jax
import jax.numpy as jnp
import numpy as np
from jax import lax

D = 2048
H = 32
DQK = 32
DV = 64
FE = 2048
TOP_K = 2
TOK_DEV = 64
SEQ = 8192
EXPERTS = 32
CAP = 5
N_EP = 32
N_TP = 4


def head_draw(key, salt_value):
    base = jax.random.fold_in(key, salt_value)
    draws = jnp.clip(1.3 * jax.random.normal(base, (SEQ, 2 * H * DQK), jnp.float32), -8.0, 8.0)
    return draws.astype(jnp.bfloat16)


def expert_draw(key, salt_value):
    base = jax.random.fold_in(key, salt_value)
    scale_factor = 3.0
    draws = scale_factor * D ** (-0.5) * jax.random.normal(base, (EXPERTS, D, FE), jnp.float32)
    return jnp.clip(draws, -1.0, 1.0).astype(jnp.bfloat16)


def draw_queries(key, part):
    return head_draw(key, 11)


def draw_key_rows(key, part):
    return head_draw(key, 12)


def draw_gate_weight(key, part):
    return expert_draw(key, 21)


def draw_up_weight(key, part):
    return expert_draw(key, 22)


def block_scale(key, dims, shards, low, top_value):
    loudness = 1.0
    for position, parts in shards:
        steps = jax.random.uniform(jax.random.fold_in(jax.random.fold_in(key, 6), position), (parts,), jnp.float32, low / len(shards), top_value / len(shards))
        loudness = loudness * jnp.repeat(jnp.exp(steps), dims[position] // parts).reshape((-1,) + (1,) * (len(dims) - 1 - position))
    return loudness


def assign_block(stream_key, own, number, rows, amount, top, most, skew):
    sequence = jax.random.permutation(stream_key, amount)
    crowded, ordinary = portions_of(amount, rows * top, most, skew, True), portions_of(amount, rows * top, most, skew, False)
    places = jnp.arange(amount)

    def named(sizes, turn):
        used = int((sizes > 0).sum())
        fixed = max(1, used // 4)
        passed = fixed + (places - fixed + turn * (used - fixed)) % max(1, amount - fixed)
        return jnp.zeros((amount,), jnp.int32).at[sequence[jnp.where(places < fixed, places, passed)]].set(jnp.asarray(sizes, jnp.int32))

    sizes = jnp.where(number % 4 == 0, named(crowded, number // 4), named(ordinary, number - number // 4 - 1))
    mixed = jax.random.permutation(jax.random.fold_in(own, 3), amount)
    donor, sink = mixed[0:amount // 2 * 2:2], mixed[1:amount // 2 * 2:2]
    room = jnp.minimum(sizes[donor] - 1, most - sizes[sink]) // 2
    room = jnp.where((donor == sequence[0]) | (sink == sequence[0]) | (sizes[sink] == 0), 0, jnp.maximum(room, 0))
    passed = jax.random.randint(jax.random.fold_in(own, 4), (amount // 2,), 0, 1 << 20) % (room + 1)
    sizes = sizes.at[donor].add(-passed).at[sink].add(passed)
    items = jnp.searchsorted(jnp.cumsum(sizes), jnp.arange(rows * top), side="right").astype(jnp.int32)
    table = items.reshape(top, rows).T
    table = table[jax.random.permutation(jax.random.fold_in(own, 1), rows)]
    turn = jax.random.randint(jax.random.fold_in(own, 2), (rows, 1), 0, top)
    return jnp.take_along_axis(table, (jnp.arange(top)[None, :] + turn) % top, axis=1)


def portions_of(number_of, total, limit, skew, full):
    loads = [(1 << 20) // math.isqrt(grade ** skew) + 1 for grade in range(1, number_of + 1)]
    largest = limit if full else min(limit, max(-(-total // number_of), total * loads[0] // sum(loads)))
    least = 1 if total - largest >= number_of - 1 else 0
    counts, rest = [largest] + [least] * (number_of - 1), total - largest - least * (number_of - 1)
    while rest > 0:
        candidates = [i for i in range(1, number_of) if counts[i] < largest] or [i for i in range(1, number_of) if counts[i] < limit]
        mass, left = sum([loads[i] for i in candidates]), rest
        for i in candidates:
            addition = min(limit - counts[i], max(1, left * loads[i] // mass), rest)
            counts[i] = counts[i] + addition
            rest = rest - addition
    return np.array(counts)


def noise(own_key, dims, spread, most, pieces=(), held_as=jnp.bfloat16):
    result = jax.random.normal(own_key, dims, jnp.float32) * spread
    if len(pieces) > 0:
        result = block_scale(own_key, dims, pieces, -0.22, 0.18) * result
    return jnp.clip(result, min=-most, max=most).astype(held_as)


def setup_inputs(seed: int = 0, part: int = 0) -> dict:
    arg_keys = jax.random.split(jax.random.key(seed), 14)
    part_splits = jax.random.split(jax.random.fold_in(arg_keys[13], part), 14)
    queries = draw_queries(jax.random.fold_in(jax.random.fold_in(arg_keys[13], part), 71), part)
    key_rows = draw_key_rows(jax.random.fold_in(jax.random.fold_in(arg_keys[13], part), 71), part)
    value_rows = noise(part_splits[2], (SEQ, H * DV), 1.0, 6.0, ((0, 32), (1, 4)))
    mix_lambda = jnp.clip(0.3 + 0.5 * jax.random.uniform(arg_keys[3], (H,), jnp.float32) ** block_scale(arg_keys[3], (H,), ((0, 4),), -0.2, 0.2), 0.3, 0.8)
    head_gain = jnp.clip(1.0 + 0.18 * jax.random.normal(arg_keys[4], (DV,), jnp.float32), 0.1, 1.9)
    out_weight = noise(arg_keys[5], (H * DV, D), (H * DV) ** -0.5, 0.125, ((0, 4),))
    expert_in = noise(part_splits[6], (SEQ, D), 1.0, 6.0, ((0, 128),))
    expert_gain = jnp.clip(1.0 + 0.18 * jax.random.normal(arg_keys[7], (D,), jnp.float32), 0.1, 1.9)
    routes_keys = jax.random.split(jax.random.fold_in(part_splits[8], 1), SEQ // TOK_DEV)
    routes_turns = jax.random.permutation(jax.random.fold_in(part_splits[8], 3), SEQ // TOK_DEV)
    routes = jax.vmap(lambda own, number: assign_block(jax.random.fold_in(part_splits[8], 2), own, number, TOK_DEV, EXPERTS, TOP_K, CAP, 1))(routes_keys, routes_turns).reshape((SEQ, TOP_K))
    route_logits = noise(part_splits[9], (SEQ, TOP_K), 1.5, 6.0, ((0, 128),), jnp.float32)
    gate_weight = draw_gate_weight(jax.random.fold_in(arg_keys[13], 71), part)
    up_weight = draw_up_weight(jax.random.fold_in(arg_keys[13], 71), part)
    down_weight = noise(arg_keys[12], (EXPERTS, FE, D), FE ** -0.5, 0.125, ((0, 32), (1, 4)))
    return dict(queries=queries, key_rows=key_rows, value_rows=value_rows, mix_lambda=mix_lambda, head_gain=head_gain, out_weight=out_weight, expert_in=expert_in, expert_gain=expert_gain, routes=routes, route_logits=route_logits, gate_weight=gate_weight, up_weight=up_weight, down_weight=down_weight)


HEAD_EPS = 0.0001
NORM_EPS = 0.1
POST_EPS = 1.0
CLAMP_LIMIT = 7.0
SIGMOID_SCALE = 1.702
OUT_SCALE = 0.8

def attend_block(query_block, key_heads, value_heads, mix_lambda, head_gain):
    scores = jnp.einsum('qhmd,khmd->hmqk', query_block.astype(jnp.float32), key_heads) * DQK ** (-0.5)
    row_max = lax.optimization_barrier(jnp.max(scores, axis=-1, keepdims=True))
    exponents = jnp.exp(scores - row_max)
    row_sums = lax.optimization_barrier(jnp.sum(exponents, axis=-1))
    weights = lax.optimization_barrier(exponents.astype(jnp.bfloat16)).astype(jnp.float32)
    attended = jnp.einsum('hmqk,khd->hmqd', weights, value_heads) / row_sums[..., None]
    differ = attended[:, 0] - mix_lambda[:, None, None] * attended[:, 1]
    normed = differ * lax.rsqrt(lax.optimization_barrier(jnp.mean(differ * differ, axis=-1, keepdims=True)) + HEAD_EPS)
    normed = (normed * head_gain * OUT_SCALE).astype(jnp.bfloat16)
    return jnp.transpose(normed, (1, 0, 2)).reshape(query_block.shape[0], H * DV)

def expert_apply(operands):
    rows_in, gate_one, up_one, down_one = operands
    gate_pre = jnp.dot(rows_in, gate_one, preferred_element_type=jnp.float32)
    up_pre = jnp.dot(rows_in, up_one, preferred_element_type=jnp.float32)
    clipped_gate = jnp.minimum(gate_pre, CLAMP_LIMIT)
    clipped_up = jnp.clip(up_pre, -CLAMP_LIMIT, CLAMP_LIMIT)
    act = (clipped_gate * jax.nn.sigmoid(SIGMOID_SCALE * clipped_gate) * (clipped_up + 1.0)).astype(jnp.bfloat16)
    block_units = FE // N_TP
    summed = jnp.zeros((rows_in.shape[0], D), jnp.float32)
    for lane_index in range(N_TP):
        lo_unit = lane_index * block_units
        partial_out = jnp.dot(act[:, lo_unit:lo_unit + block_units], down_one[lo_unit:lo_unit + block_units], preferred_element_type=jnp.float32)
        summed = summed + lax.optimization_barrier(partial_out.astype(jnp.bfloat16)).astype(jnp.float32)
    return summed.astype(jnp.bfloat16)

def reference(queries, key_rows, value_rows, mix_lambda, head_gain, out_weight, expert_in, expert_gain, routes, route_logits, gate_weight, up_weight, down_weight):
    query_len = math.gcd(SEQ, 128)
    key_heads = key_rows.astype(jnp.float32).reshape(SEQ, H, 2, DQK)
    value_heads = value_rows.astype(jnp.float32).reshape(SEQ, H, DV)
    query_blocks = queries.reshape(SEQ // query_len, query_len, H, 2, DQK)
    head_rows = lax.map(lambda block: attend_block(block, key_heads, value_heads, mix_lambda, head_gain), query_blocks).reshape(SEQ, H * DV)
    mixer_out = jnp.dot(head_rows, out_weight, preferred_element_type=jnp.float32).astype(jnp.bfloat16)
    inputs_wide = expert_in.astype(jnp.float32)
    normed = inputs_wide * lax.rsqrt(lax.optimization_barrier(jnp.mean(inputs_wide * inputs_wide, axis=-1, keepdims=True)) + NORM_EPS)
    normed = (normed * expert_gain).astype(jnp.bfloat16)
    route_weight = 1.0 / lax.optimization_barrier(jnp.sum(jnp.exp(route_logits[:, None, :] - route_logits[:, :, None]), axis=-1))
    flat_routes = routes.reshape(-1).astype(jnp.int32)
    token_ids = (jnp.arange(SEQ * TOP_K, dtype=jnp.int32) // TOP_K).astype(jnp.int32)
    onehot_table = (flat_routes[:, None] == jnp.arange(EXPERTS, dtype=jnp.int32)[None, :]).astype(jnp.int32)
    ranks = jnp.cumsum(onehot_table, axis=0) - onehot_table
    positions = lax.optimization_barrier(jnp.sum(ranks * onehot_table, axis=1)).astype(jnp.int32)
    slot_total = N_EP * N_TP * CAP
    buffers = jnp.zeros((EXPERTS, slot_total, D), jnp.bfloat16)
    buffers = buffers.at[flat_routes, positions].set(normed[token_ids])
    results = lax.map(expert_apply, (buffers, gate_weight, up_weight, down_weight))
    picked = results[flat_routes, positions].astype(jnp.float32).reshape(SEQ, TOP_K, D)
    combined = lax.optimization_barrier(jnp.sum(route_weight[..., None] * picked, axis=1))
    expert_out = combined * lax.rsqrt(lax.optimization_barrier(jnp.mean(combined * combined, axis=-1, keepdims=True)) + POST_EPS)
    return (mixer_out, expert_out.astype(jnp.bfloat16))
```

```python
import functools
import math

import jax
import jax.numpy as jnp
from jax import lax
from jax.experimental import pallas as pl
from jax.experimental.pallas import tpu as pltpu
from jax.sharding import PartitionSpec as P

DQK = 32
DV = 64
HEAD_EPS = 0.0001
NORM_EPS = 0.1
POST_EPS = 1.0
CLAMP_LIMIT = 7.0
SIGMOID_SCALE = 1.702
OUT_SCALE = 0.8
CEXP = DQK ** -0.5 * math.log2(math.e)
LANES = 128
GROUP = 256
ONES = 16
LOOK = 2
MESH = pl.DeviceIdType.MESH
F32, BF16 = jnp.float32, jnp.bfloat16
K, V = 0, 1
R, L = 0, 1


def dot(a, b):
    return jnp.dot(a, b, preferred_element_type=F32)


def kernel(
    n_ep, n_tp, cap, stages,
    q_ref, k_ref, v_ref, lam_ref, gain_ref, x_ref, eg_ref, routes_ref, logit_ref,
    ow_hbm, gw_hbm, uw_hbm, dw_hbm,
    mix_ref, eo_ref,
    kbuf, vbuf, q_mask, m_ref, acc_ref,
    gw, uw, dw, ow,
    wide, packed, landed, xrows, act, part, precv, returned, comb, hr_ref, mp, mrecv,
    wsem, d_send, d_recv, r_send, r_recv, b_send, b_recv,
    x_send, x_recv, p_send, p_recv, e_send, e_recv, m_send, m_recv,
):
    ep, tp = lax.axis_index("ep"), lax.axis_index("tp")
    n_z = n_ep // 2
    half = n_z // 2
    z, core = ep // 2, lax.rem(ep, 2)
    sibling = 2 * z + 1 - core
    rows = q_ref.shape[0]
    heads = q_ref.shape[1] // (2 * DQK)
    maps = 2 * heads
    tokens, width = x_ref.shape
    n_lane = width // LANES
    slots = n_ep * cap
    fe = gw.shape[1]

    weight_copies = [
        pltpu.make_async_copy(src, dst, wsem.at[i])
        for i, (src, dst) in enumerate(((gw_hbm, gw), (uw_hbm, uw), (dw_hbm, dw), (ow_hbm, ow)))
    ]
    for copy in weight_copies:
        copy.start()

    barrier = pltpu.get_barrier_semaphore()

    def greet_ep(d, _):
        pl.semaphore_signal(barrier, inc=1, device_id={"ep": lax.rem(ep + d, n_ep)}, device_id_type=MESH)
        return 0

    def greet_tp(d, _):
        pl.semaphore_signal(barrier, inc=1, device_id={"tp": lax.rem(tp + d, n_tp)}, device_id_type=MESH)
        return 0

    lax.fori_loop(1, n_ep, greet_ep, 0)
    lax.fori_loop(1, n_tp, greet_tp, 0)

    routes = routes_ref[...].astype(F32)
    first, second = routes[:, 0:1], routes[:, 1:2]
    experts = lax.broadcasted_iota(jnp.int32, (tokens, n_ep), 1).astype(F32)
    is_first = (first == experts).astype(F32)
    is_second = (second == experts).astype(F32)
    earlier = (
        lax.broadcasted_iota(jnp.int32, (tokens, tokens), 0)
        > lax.broadcasted_iota(jnp.int32, (tokens, tokens), 1)
    ).astype(BF16)
    ahead = dot(earlier, (is_first + is_second).astype(BF16))
    slot_first = first * cap + jnp.sum(ahead * is_first, axis=1, keepdims=True)
    slot_second = second * cap + jnp.sum(ahead * is_second, axis=1, keepdims=True)

    def picks(slot, count):
        grid = lax.broadcasted_iota(jnp.int32, (tokens, count), 1).astype(F32)
        return (slot == grid).astype(BF16)

    x = x_ref[...].astype(F32)
    normed = x * lax.rsqrt(jnp.mean(x * x, axis=-1, keepdims=True) + NORM_EPS)
    normed = (normed * eg_ref[...]).astype(BF16)
    padded = -(-slots // LANES) * LANES
    placing = (picks(slot_first, padded) + picks(slot_second, padded)).astype(BF16)

    def to_tiles(j, columns):
        wide[pl.ds(j, slots, stride=n_lane), :] = columns

    step_cols = min(width, 512)
    for c0 in range(0, width, step_cols):
        placed = lax.dot_general(
            placing, normed[:, c0 : c0 + step_cols], (((0,), (0,)), ((), ())),
            preferred_element_type=F32,
        )
        for c1 in range(0, step_cols, LANES):
            to_tiles((c0 + c1) // LANES, placed[:slots, c1 : c1 + LANES])

    def pack_tiles(dst):
        def one(i, _):
            block = wide[pl.ds(pl.multiple_of(i * cap * n_lane, n_lane), cap * n_lane), :]
            dst[pl.ds(i * cap, cap)] = block.reshape(cap, n_lane, LANES).astype(BF16)
            return 0

        lax.fori_loop(0, n_ep, one, 0)

    def unpack_tiles(src):
        def one(i, _):
            block = src[pl.ds(i * cap, cap)].astype(F32)
            wide[pl.ds(pl.multiple_of(i * cap * n_lane, n_lane), cap * n_lane), :] = block.reshape(cap * n_lane, LANES)
            return 0

        lax.fori_loop(0, n_ep, one, 0)

    pack_tiles(packed)

    kbuf[ep] = k_ref[...]
    vbuf[ep] = v_ref[...].astype(F32).T.astype(BF16)
    q_cols = q_ref[...].astype(F32).T
    row_map = lax.broadcasted_iota(jnp.int32, (GROUP, rows), 0) // DQK
    per_group = GROUP // DQK
    for hm in range(maps):
        g = hm // per_group
        block = q_cols[GROUP * g : GROUP * g + GROUP]
        q_mask[hm] = jnp.where(row_map == hm % per_group, block, 0.0).astype(BF16)
        m_ref[hm] = jnp.full((1, rows), -1e30, F32)
        acc_ref[hm] = jnp.zeros((DV + ONES, rows), F32)

    pl.semaphore_wait(barrier, n_ep - 1 + n_tp - 1)

    def slot_copy(src, dst, send, recv, d):
        to = lax.rem(ep + d, n_ep)
        return pltpu.make_async_remote_copy(
            src_ref=src.at[pl.ds(to * cap, cap)],
            dst_ref=dst.at[pl.ds(ep * cap, cap)],
            send_sem=send.at[d], recv_sem=recv.at[d],
            device_id={"ep": to}, device_id_type=MESH,
        )

    def slot_arrival(dst, send, recv, d):
        source = lax.rem(ep + n_ep - d, n_ep)
        here = dst.at[pl.ds(source * cap, cap)]
        return pltpu.make_async_remote_copy(
            src_ref=here, dst_ref=here, send_sem=send.at[d], recv_sem=recv.at[d],
            device_id={"ep": source}, device_id_type=MESH,
        )

    def send_slots(src, dst, send, recv):
        def pair(i, _):
            slot_copy(src, dst, send, recv, i).start()
            slot_copy(src, dst, send, recv, n_ep - i).start()
            return 0

        lax.fori_loop(1, n_ep // 2, pair, 0)
        slot_copy(src, dst, send, recv, n_ep // 2).start()
        dst[pl.ds(ep * cap, cap)] = src[pl.ds(ep * cap, cap)]

    def take_slots(dst, send, recv):
        def one(d, _):
            slot_arrival(dst, send, recv, d).wait_recv()
            return 0

        lax.fori_loop(1, n_ep, one, 0)

    def flush_slots(src, dst, send, recv):
        def one(d, _):
            slot_copy(src, dst, send, recv, d).wait_send()
            return 0

        lax.fori_loop(1, n_ep, one, 0)

    send_slots(packed, landed, d_send, d_recv)

    bufs = (kbuf, vbuf)
    limits = ((half, half - 1), (half - 1, half))

    def block_at(direction, s):
        return lax.rem(z + n_z - s, n_z) if direction == R else lax.rem(z + s, n_z)

    def ring_copy(a, direction, s):
        there = bufs[a].at[2 * block_at(direction, s - 1) + core]
        to = lax.rem(ep + 2, n_ep) if direction == R else lax.rem(ep + n_ep - 2, n_ep)
        return pltpu.make_async_remote_copy(
            src_ref=there, dst_ref=there,
            send_sem=r_send.at[a, direction, s], recv_sem=r_recv.at[a, direction, s],
            device_id={"ep": to}, device_id_type=MESH,
        )

    def ring_arrival(a, direction, s):
        here = bufs[a].at[2 * block_at(direction, s) + core]
        source = lax.rem(ep + n_ep - 2, n_ep) if direction == R else lax.rem(ep + 2, n_ep)
        return pltpu.make_async_remote_copy(
            src_ref=here, dst_ref=here,
            send_sem=r_send.at[a, direction, s], recv_sem=r_recv.at[a, direction, s],
            device_id={"ep": source}, device_id_type=MESH,
        )

    def across(a, direction, s, owner):
        here = bufs[a].at[2 * block_at(direction, s) + owner]
        return pltpu.make_async_remote_copy(
            src_ref=here, dst_ref=here,
            send_sem=b_send.at[a, direction, s], recv_sem=b_recv.at[a, direction, s],
            device_id={"ep": sibling}, device_id_type=MESH,
        )

    for a in (K, V):
        for direction in (R, L):
            ring_copy(a, direction, 1).start()
        across(a, R, 0, core).start()

    def hop(a, direction, s):
        limit = limits[a][direction]

        @pl.when(s <= limit)
        def _():
            ring_arrival(a, direction, s).wait_recv()

            @pl.when(s < limit)
            def _():
                ring_copy(a, direction, s + 1).start()

            across(a, direction, s, core).start()

    def absorb_chip(chip):
        ones = jnp.ones((ONES, 2 * rows), BF16)

        def score(hm):
            c0 = GROUP * (hm // per_group)
            keys = jnp.concatenate([kbuf[2 * chip + b, :, c0 : c0 + GROUP] for b in (0, 1)], axis=0)
            return dot(keys, q_mask[hm])

        def values(h):
            cols = [vbuf[2 * chip + b, DV * h : DV * h + DV, :] for b in (0, 1)]
            return jnp.concatenate([jnp.concatenate(cols, axis=1), ones], axis=0)

        pending = [score(i) for i in range(min(LOOK, maps))]
        for hm in range(maps):
            if hm + LOOK < maps:
                pending.append(score(hm + LOOK))
            s = pending.pop(0)
            m_old = m_ref[hm]
            m_new = jnp.maximum(m_old, jnp.max(s, axis=0, keepdims=True))
            weights = jnp.exp2(s * CEXP - m_new * CEXP).astype(BF16)
            shrink = jnp.exp2((m_old - m_new) * CEXP)
            acc_ref[hm] = acc_ref[hm] * shrink + dot(values(hm // 2), weights)
            m_ref[hm] = m_new

    def tp_copy(src, dst, to, send, recv):
        return pltpu.make_async_remote_copy(
            src_ref=src, dst_ref=dst, send_sem=send, recv_sem=recv,
            device_id={"tp": to}, device_id_type=MESH,
        )

    def up(i):
        return lax.rem(tp + i, n_tp)

    def down(i):
        return lax.rem(tp + n_tp - i, n_tp)

    def x_copy(i):
        return tp_copy(xrows.at[tp], xrows.at[tp], up(i), x_send.at[i], x_recv.at[i])

    def stage_rows():
        take_slots(landed, d_send, d_recv)
        unpack_tiles(landed)
        for j in range(n_lane):
            xrows[tp, :, j * LANES : (j + 1) * LANES] = wide[pl.ds(j, slots, stride=n_lane), :].astype(BF16)
        for i in range(1, n_tp):
            x_copy(i).start()

    def p_copy(i):
        return tp_copy(part.at[down(i)], precv.at[tp], down(i), p_send.at[i], p_recv.at[i])

    def p_arrival(i):
        here = precv.at[up(i)]
        return tp_copy(here, here, up(i), p_send.at[i], p_recv.at[i])

    def stage_experts():
        for copy in weight_copies[:3]:
            copy.wait()

        def one(i, _):
            source = down(i)

            @pl.when(i > 0)
            def _():
                here = xrows.at[source]
                tp_copy(here, here, source, x_send.at[i], x_recv.at[i]).wait_recv()

            x_in = xrows[source]
            cols = min(fe, 256)
            for c0 in range(0, fe, cols):
                gate = jnp.minimum(dot(x_in, gw[:, c0 : c0 + cols]), CLAMP_LIMIT)
                lift = jnp.clip(dot(x_in, uw[:, c0 : c0 + cols]), -CLAMP_LIMIT, CLAMP_LIMIT)
                act[:, c0 : c0 + cols] = (gate * jax.nn.sigmoid(SIGMOID_SCALE * gate) * (lift + 1.0)).astype(BF16)
            for c0 in range(0, width, step_cols):
                part[source, :, c0 : c0 + step_cols] = dot(act[...], dw[:, c0 : c0 + step_cols]).astype(BF16)

            @pl.when(i > 0)
            def _():
                p_copy(i).start()

            return 0

        lax.fori_loop(0, n_tp, one, 0)

    def stage_return():
        flush_slots(packed, landed, d_send, d_recv)
        for i in range(1, n_tp):
            p_arrival(i).wait_recv()
        for j in range(n_lane):
            c = slice(j * LANES, (j + 1) * LANES)
            total = part[tp, :, c].astype(F32)
            for i in range(1, n_tp):
                total = total + precv[up(i), :, c].astype(F32)
            to_tiles(j, total)
        pack_tiles(packed)
        send_slots(packed, returned, e_send, e_recv)

    def step(t, _):
        s = t // 2 + 1
        u = lax.rem(t, 2)

        @pl.when(u == 0)
        def _():
            hop(K, R, s)
            hop(K, L, s)

        @pl.when(u == 1)
        def _():
            hop(V, R, s)
            hop(V, L, s)

        done = s - 1

        @pl.when(jnp.logical_and(u == 0, done < half))
        def _():
            across(K, R, done, 1 - core).wait_recv()
            across(V, R, done, 1 - core).wait_recv()

        @pl.when(jnp.logical_and(u == 1, done > 0))
        def _():
            across(K, L, done, 1 - core).wait_recv()
            across(V, L, done, 1 - core).wait_recv()

        @pl.when(t == 2 * half)
        def _():
            across(K, R, half, 1 - core).wait_recv()
            across(V, L, half, 1 - core).wait_recv()

        @pl.when(t != 1)
        def _():
            absorb_chip(lax.rem(z + n_z + jnp.where(u == 0, -done, done), n_z))

        @pl.when(t == stages[0])
        def _():
            stage_rows()

        @pl.when(t == stages[1])
        def _():
            stage_experts()

        @pl.when(t == stages[2])
        def _():
            stage_return()

        return 0

    lax.fori_loop(0, 2 * half + 1, step, 0)

    for h in range(heads):
        one = acc_ref[2 * h, 0:DV] / acc_ref[2 * h, DV : DV + 1]
        two = acc_ref[2 * h + 1, 0:DV] / acc_ref[2 * h + 1, DV : DV + 1]
        differ = one - lam_ref[h] * two
        scale = lax.rsqrt(jnp.mean(differ * differ, axis=0, keepdims=True) + HEAD_EPS)
        hr_ref[DV * h : DV * h + DV, :] = differ * scale * gain_ref[...] * OUT_SCALE
    weight_copies[3].wait()
    head_rows = hr_ref[...].T.astype(BF16)
    for c0 in range(0, width, step_cols):
        share = dot(head_rows, ow[:, c0 : c0 + step_cols]).astype(BF16)
        for d in range(n_tp):
            mp[d, :, c0 : c0 + step_cols] = share[tokens * d : tokens * (d + 1)]

    def m_copy(i):
        return tp_copy(mp.at[up(i)], mrecv.at[tp], up(i), m_send.at[i], m_recv.at[i])

    def m_arrival(i):
        here = mrecv.at[down(i)]
        return tp_copy(here, here, down(i), m_send.at[i], m_recv.at[i])

    for i in range(1, n_tp):
        m_copy(i).start()

    take_slots(returned, e_send, e_recv)
    unpack_tiles(returned)
    for j in range(n_lane):
        comb[:, j * LANES : (j + 1) * LANES] = wide[pl.ds(j, slots, stride=n_lane), :].astype(BF16)
    logits = logit_ref[...]
    low, high = logits[:, 0:1], logits[:, 1:2]
    combined = dot(picks(slot_first, slots), comb[...]) * (1.0 / (1.0 + jnp.exp(high - low)))
    combined = combined + dot(picks(slot_second, slots), comb[...]) * (1.0 / (jnp.exp(low - high) + 1.0))
    post = lax.rsqrt(jnp.mean(combined * combined, axis=-1, keepdims=True) + POST_EPS)
    eo_ref[...] = (combined * post).astype(BF16)

    for i in range(1, n_tp):
        m_arrival(i).wait_recv()
    mixed = mp[tp].astype(F32)
    for i in range(1, n_tp):
        mixed = mixed + mrecv[down(i)].astype(F32)
    mix_ref[...] = mixed.astype(BF16)

    flush_slots(packed, returned, e_send, e_recv)
    for i in range(1, n_tp):
        x_copy(i).wait_send()
        p_copy(i).wait_send()
        m_copy(i).wait_send()
    for a in (K, V):
        across(a, R, 0, core).wait_send()
        for direction in (R, L):

            def gone(s, _, a=a, direction=direction):
                ring_copy(a, direction, s).wait_send()
                across(a, direction, s, core).wait_send()
                return 0

            lax.fori_loop(1, limits[a][direction] + 1, gone, 0)


def local(
    n_ep, n_tp,
    queries, key_rows, value_rows, mix_lambda, head_gain, out_weight, expert_in, expert_gain,
    routes, route_logits, gate_weight, up_weight, down_weight,
):
    rows, cols = queries.shape
    heads = cols // (2 * DQK)
    tokens, width = expert_in.shape
    fe = gate_weight.shape[2]
    top = routes.shape[1]
    cap = (5 * tokens * top + 4 * n_ep - 1) // (4 * n_ep)
    slots = n_ep * cap
    n_lane = width // LANES
    half = n_ep // 4
    last = 2 * half
    stages = (min(2, last), min(6, last), min(11, last))
    dma = pltpu.SemaphoreType.DMA
    vmem = pl.BlockSpec(memory_space=pltpu.VMEM)
    whole = pl.BlockSpec(memory_space=pl.ANY)
    out = jax.ShapeDtypeStruct((tokens, width), BF16)
    return pl.pallas_call(
        functools.partial(kernel, n_ep, n_tp, cap, stages),
        out_shape=(out, out),
        in_specs=[vmem, vmem, vmem, pl.BlockSpec(memory_space=pltpu.SMEM), vmem, vmem, vmem, vmem, vmem]
        + [whole] * 4,
        out_specs=(vmem, vmem),
        scratch_shapes=[
            pltpu.VMEM((n_ep, rows, cols), BF16),
            pltpu.VMEM((n_ep, heads * DV, rows), BF16),
            pltpu.VMEM((2 * heads, GROUP, rows), BF16),
            pltpu.VMEM((2 * heads, 1, rows), F32),
            pltpu.VMEM((2 * heads, DV + ONES, rows), F32),
            pltpu.VMEM((width, fe), BF16),
            pltpu.VMEM((width, fe), BF16),
            pltpu.VMEM((fe, width), BF16),
            pltpu.VMEM(out_weight.shape, BF16),
            pltpu.VMEM((slots * n_lane, LANES), F32),
            pltpu.VMEM((slots, n_lane, LANES), BF16),
            pltpu.VMEM((slots, n_lane, LANES), BF16),
            pltpu.VMEM((n_tp, slots, width), BF16),
            pltpu.VMEM((slots, fe), BF16),
            pltpu.VMEM((n_tp, slots, width), BF16),
            pltpu.VMEM((n_tp, slots, width), BF16),
            pltpu.VMEM((slots, n_lane, LANES), BF16),
            pltpu.VMEM((slots, width), BF16),
            pltpu.VMEM((heads * DV, rows), F32),
            pltpu.VMEM((n_tp, tokens, width), BF16),
            pltpu.VMEM((n_tp, tokens, width), BF16),
            dma((4,)),
            dma((n_ep,)), dma((n_ep,)),
            dma((2, 2, half + 1)), dma((2, 2, half + 1)),
            dma((2, 2, half + 1)), dma((2, 2, half + 1)),
            dma((n_tp,)), dma((n_tp,)),
            dma((n_tp,)), dma((n_tp,)),
            dma((n_ep,)), dma((n_ep,)),
            dma((n_tp,)), dma((n_tp,)),
        ],
        compiler_params=pltpu.CompilerParams(
            collective_id=0, has_side_effects=True, vmem_limit_bytes=63 * 1024 * 1024
        ),
        name="mixer_and_experts",
    )(
        queries, key_rows, value_rows, mix_lambda, head_gain.reshape(DV, 1), expert_in,
        expert_gain.reshape(1, width), routes, route_logits, out_weight,
        gate_weight[0], up_weight[0], down_weight[0],
    )


def solution(mesh):
    every = ("grp", "ep", "tp")
    return jax.shard_map(
        functools.partial(local, mesh.shape["ep"], mesh.shape["tp"]),
        mesh=mesh,
        in_specs=(
            P(("grp", "ep"), "tp"), P(("grp", "ep"), "tp"), P(("grp", "ep"), "tp"),
            P("tp"), P(), P("tp", None), P(every, None), P(), P(every, None), P(every, None),
            P("ep", None, "tp"), P("ep", None, "tp"), P("ep", "tp", None),
        ),
        out_specs=(P(every, None), P(every, None)),
        check_vma=False,
    )
```

```python
import functools
import math

import jax
import jax.numpy as jnp
from jax import lax
from jax.experimental import pallas as pl
from jax.experimental.pallas import tpu as pltpu
from jax.sharding import PartitionSpec as P

DQK = 32
DV = 64
HEAD_EPS = 0.0001
NORM_EPS = 0.1
POST_EPS = 1.0
CLAMP_LIMIT = 7.0
SIGMOID_SCALE = 1.702
OUT_SCALE = 0.8
CEXP = DQK ** -0.5 * math.log2(math.e)
LANES = 128
PAIR = 2 * DQK + DV
ONES = 16
LOOK = 2
MESH = pl.DeviceIdType.MESH
F32, BF16 = jnp.float32, jnp.bfloat16


def dot(a, b):
    return jnp.dot(a, b, preferred_element_type=F32)


def kernel(
    n_ep, n_tp, cap, stages,
    q_ref, k_ref, v_ref, lam_ref, gain_ref, x_ref, eg_ref, routes_ref, logit_ref,
    ow_hbm, gw_hbm, uw_hbm, dw_hbm,
    mix_ref, eo_ref,
    kv_out, kv_in, q_out, q_in, q_mask, vt_ref, m_ref, acc_ref, h_out, h_in,
    gw, uw, dw, ow,
    wide, packed, landed, xrows, act, part, precv, returned, comb, mp, mrecv,
    wsem, d_send, d_recv, q_send, q_recv, k_send, k_recv, f_send, b_send, b_recv, h_send, h_recv,
    x_send, x_recv, p_send, p_recv, e_send, e_recv, m_send, m_recv,
):
    ep, tp = lax.axis_index("ep"), lax.axis_index("tp")
    n_z = n_ep // 2
    depth = n_z // 2
    z, core = ep // 2, lax.rem(ep, 2)
    sibling = 2 * z + 1 - core
    head, odd = z // 2, lax.rem(z, 2)
    partner = z + 1 - 2 * odd
    parts = n_ep // 4
    quarter = ep // parts
    rows = q_ref.shape[0]
    heads = q_ref.shape[1] // (2 * DQK)
    units = 2 * parts
    tokens, width = x_ref.shape
    n_lane = width // LANES
    slots = n_ep * cap
    fe = gw.shape[1]

    weight_copies = [
        pltpu.make_async_copy(src, dst, wsem.at[i])
        for i, (src, dst) in enumerate(((gw_hbm, gw), (uw_hbm, uw), (dw_hbm, dw), (ow_hbm, ow)))
    ]
    for copy in weight_copies:
        copy.start()

    barrier = pltpu.get_barrier_semaphore()

    def greet_ep(d, _):
        pl.semaphore_signal(barrier, inc=1, device_id={"ep": lax.rem(ep + d, n_ep)}, device_id_type=MESH)
        return 0

    def greet_tp(d, _):
        pl.semaphore_signal(barrier, inc=1, device_id={"tp": lax.rem(tp + d, n_tp)}, device_id_type=MESH)
        return 0

    lax.fori_loop(1, n_ep, greet_ep, 0)
    lax.fori_loop(1, n_tp, greet_tp, 0)

    routes = routes_ref[...].astype(F32)
    first, second = routes[0:1], routes[1:2]
    experts = lax.broadcasted_iota(jnp.int32, (n_ep, tokens), 0).astype(F32)
    is_first = (first == experts).astype(F32)
    is_second = (second == experts).astype(F32)
    earlier = (
        lax.broadcasted_iota(jnp.int32, (tokens, tokens), 0)
        < lax.broadcasted_iota(jnp.int32, (tokens, tokens), 1)
    ).astype(BF16)
    ahead = dot((is_first + is_second).astype(BF16), earlier)
    slot_first = first * cap + jnp.sum(ahead * is_first, axis=0, keepdims=True)
    slot_second = second * cap + jnp.sum(ahead * is_second, axis=0, keepdims=True)

    def picks(slot):
        grid = lax.broadcasted_iota(jnp.int32, (slots, tokens), 0).astype(F32)
        return (slot == grid).astype(BF16)

    def column(row):
        n = row.shape[1]
        eye = lax.broadcasted_iota(jnp.int32, (n, n), 0) == lax.broadcasted_iota(jnp.int32, (n, n), 1)
        return jnp.sum(jnp.where(eye, row, 0.0), axis=1, keepdims=True)

    x = x_ref[...].astype(F32)
    normed = x * lax.rsqrt(jnp.mean(x * x, axis=-1, keepdims=True) + NORM_EPS)
    normed = (normed * eg_ref[...]).astype(BF16)
    placing = picks(slot_first) + picks(slot_second)

    def to_tiles(j, columns):
        wide[pl.ds(j, slots, stride=n_lane), :] = columns

    step_cols = min(width, 512)
    for c0 in range(0, width, step_cols):
        placed = dot(placing, normed[:, c0 : c0 + step_cols])
        for c1 in range(0, step_cols, LANES):
            to_tiles((c0 + c1) // LANES, placed[:, c1 : c1 + LANES])

    def pack_tiles(dst):
        def one(i, _):
            block = wide[pl.ds(pl.multiple_of(i * cap * n_lane, n_lane), cap * n_lane), :]
            dst[pl.ds(i * cap, cap)] = block.reshape(cap, n_lane, LANES).astype(BF16)
            return 0

        lax.fori_loop(0, n_ep, one, 0)

    def unpack_tiles(src):
        def one(i, _):
            block = src[pl.ds(i * cap, cap)].astype(F32)
            wide[pl.ds(pl.multiple_of(i * cap * n_lane, n_lane), cap * n_lane), :] = block.reshape(cap * n_lane, LANES)
            return 0

        lax.fori_loop(0, n_ep, one, 0)

    pack_tiles(packed)

    q_out[...] = q_ref[...].astype(F32).T.reshape(heads, 2 * DQK, rows).astype(BF16)
    for h in range(heads):
        c = slice(DV * h, DV * h + DV)
        kv_out[h] = jnp.concatenate([k_ref[:, c].astype(F32), v_ref[:, c].astype(F32)], axis=1).astype(BF16)
    vt_ref[DV:, :] = jnp.ones((ONES, 2 * rows), BF16)
    for u in range(units):
        m_ref[u] = jnp.full((1, rows), -1e30, F32)
        acc_ref[u] = jnp.zeros((DV + ONES, rows), F32)

    pl.semaphore_wait(barrier, n_ep - 1 + n_tp - 1)

    def slot_copy(src, dst, send, recv, d):
        to = lax.rem(ep + d, n_ep)
        return pltpu.make_async_remote_copy(
            src_ref=src.at[pl.ds(to * cap, cap)],
            dst_ref=dst.at[pl.ds(ep * cap, cap)],
            send_sem=send.at[d], recv_sem=recv.at[d],
            device_id={"ep": to}, device_id_type=MESH,
        )

    def slot_arrival(dst, send, recv, d):
        source = lax.rem(ep + n_ep - d, n_ep)
        here = dst.at[pl.ds(source * cap, cap)]
        return pltpu.make_async_remote_copy(
            src_ref=here, dst_ref=here, send_sem=send.at[d], recv_sem=recv.at[d],
            device_id={"ep": source}, device_id_type=MESH,
        )

    def send_slots(src, dst, send, recv):
        def pair(i, _):
            slot_copy(src, dst, send, recv, i).start()
            slot_copy(src, dst, send, recv, n_ep - i).start()
            return 0

        lax.fori_loop(1, n_ep // 2, pair, 0)
        slot_copy(src, dst, send, recv, n_ep // 2).start()
        dst[pl.ds(ep * cap, cap)] = src[pl.ds(ep * cap, cap)]

    def take_slots(dst, send, recv):
        def one(d, _):
            slot_arrival(dst, send, recv, d).wait_recv()
            return 0

        lax.fori_loop(1, n_ep, one, 0)

    def flush_slots(src, dst, send, recv):
        def one(d, _):
            slot_copy(src, dst, send, recv, d).wait_send()
            return 0

        lax.fori_loop(1, n_ep, one, 0)

    def remote(src, dst, send, recv, to):
        return pltpu.make_async_remote_copy(
            src_ref=src, dst_ref=dst, send_sem=send, recv_sem=recv,
            device_id={"ep": to}, device_id_type=MESH,
        )

    def each(count, act_on, body, own):
        def one(i, _):
            @pl.when(act_on(i) != ep)
            def _():
                body(i)

            if own is not None:

                @pl.when(act_on(i) == ep)
                def _():
                    own(i)

            return 0

        lax.fori_loop(0, count, one, 0)

    def attends(h):
        return 4 * h + quarter

    def asks(i):
        return parts * lax.rem(ep, 4) + i

    def q_copy(h):
        return remote(q_out.at[h], q_in.at[lax.rem(ep, parts)], q_send.at[h], q_recv.at[lax.rem(ep, parts)], attends(h))

    def q_arrival(i):
        return remote(q_in.at[i], q_in.at[i], q_send.at[0], q_recv.at[i], asks(i))

    def q_own(h):
        q_in[lax.rem(ep, parts)] = q_out[h]

    each(heads, attends, lambda h: q_copy(h).start(), q_own)

    def kv_copy(j):
        pair = lax.rem(head + j, heads)
        rightward = 2 * j - odd < depth
        to = 2 * pair + jnp.where(rightward, 0, 1)
        return remote(kv_out.at[pair], kv_in.at[ep], k_send.at[j], k_recv.at[z], 2 * to + core)

    def side(k):
        return lax.rem(z + n_z + jnp.where(odd == 1, k, -k), n_z)

    def far_side(k):
        return lax.rem(partner + n_z + jnp.where(odd == 1, -k, k), n_z)

    def kv_arrival(chip):
        here = kv_in.at[2 * chip + core]
        return remote(here, here, k_send.at[0], k_recv.at[chip], 2 * partner + core)

    def onward(chip):
        here = kv_in.at[2 * chip + core]
        return remote(here, here, f_send.at[chip], k_recv.at[chip], 2 * partner + core)

    def across(chip, owner):
        here = kv_in.at[2 * chip + owner]
        return remote(here, here, b_send.at[chip], b_recv.at[chip], sibling)

    kv_in[ep] = kv_out[head]
    for j in (1, heads - 1):
        if heads > 2 or j == 1:
            kv_copy(j).start()
        if heads == 2:
            break
    onward(z).start()
    across(z, core).start()
    send_slots(packed, landed, d_send, d_recv)

    def kv_rest(j, _):
        kv_copy(j).start()
        kv_copy(heads - j).start()
        return 0

    if heads > 2:
        lax.fori_loop(2, heads // 2, kv_rest, 0)
        kv_copy(heads // 2).start()

    each(parts, asks, lambda i: q_arrival(i).wait_recv(), None)
    row_map = lax.broadcasted_iota(jnp.int32, (PAIR, rows), 0) // DQK

    def mask_queries(i, _):
        block = jnp.concatenate([q_in[i].astype(F32), jnp.zeros((DV, rows), F32)], axis=0)
        for m in (0, 1):
            q_mask[2 * i + m] = jnp.where(row_map == m, block, 0.0).astype(BF16)
        return 0

    lax.fori_loop(0, parts, mask_queries, 0)

    def absorb_chip(chip):
        for b in (0, 1):
            turned = kv_in[2 * chip + b].astype(F32).T
            vt_ref[0:DV, b * rows : (b + 1) * rows] = turned[2 * DQK :].astype(BF16)

        def score(u):
            keys = jnp.concatenate([kv_in[2 * chip + b] for b in (0, 1)], axis=0)
            return dot(keys, q_mask[u])

        pending = [score(i) for i in range(min(LOOK, units))]
        for u in range(units):
            if u + LOOK < units:
                pending.append(score(u + LOOK))
            s = pending.pop(0)
            m_old = m_ref[u]
            m_new = jnp.maximum(m_old, jnp.max(s, axis=0, keepdims=True))
            weights = jnp.exp2(s * CEXP - m_new * CEXP).astype(BF16)
            shrink = jnp.exp2((m_old - m_new) * CEXP)
            acc_ref[u] = acc_ref[u] * shrink + dot(vt_ref[...], weights)
            m_ref[u] = m_new

    def tp_copy(src, dst, to, send, recv):
        return pltpu.make_async_remote_copy(
            src_ref=src, dst_ref=dst, send_sem=send, recv_sem=recv,
            device_id={"tp": to}, device_id_type=MESH,
        )

    def up(i):
        return lax.rem(tp + i, n_tp)

    def down(i):
        return lax.rem(tp + n_tp - i, n_tp)

    def x_copy(i):
        return tp_copy(xrows.at[tp], xrows.at[tp], up(i), x_send.at[i], x_recv.at[i])

    def stage_rows():
        take_slots(landed, d_send, d_recv)
        unpack_tiles(landed)
        for j in range(n_lane):
            xrows[tp, :, j * LANES : (j + 1) * LANES] = wide[pl.ds(j, slots, stride=n_lane), :].astype(BF16)
        for i in range(1, n_tp):
            x_copy(i).start()

    def p_copy(i):
        return tp_copy(part.at[down(i)], precv.at[tp], down(i), p_send.at[i], p_recv.at[i])

    def p_arrival(i):
        here = precv.at[up(i)]
        return tp_copy(here, here, up(i), p_send.at[i], p_recv.at[i])

    def stage_experts():
        for copy in weight_copies[:3]:
            copy.wait()

        def one(i, _):
            source = down(i)

            @pl.when(i > 0)
            def _():
                here = xrows.at[source]
                tp_copy(here, here, source, x_send.at[i], x_recv.at[i]).wait_recv()

            x_in = xrows[source]
            cols = min(fe, 256)
            for c0 in range(0, fe, cols):
                gate = jnp.minimum(dot(x_in, gw[:, c0 : c0 + cols]), CLAMP_LIMIT)
                lift = jnp.clip(dot(x_in, uw[:, c0 : c0 + cols]), -CLAMP_LIMIT, CLAMP_LIMIT)
                act[:, c0 : c0 + cols] = (gate * jax.nn.sigmoid(SIGMOID_SCALE * gate) * (lift + 1.0)).astype(BF16)
            for c0 in range(0, width, step_cols):
                part[source, :, c0 : c0 + step_cols] = dot(act[...], dw[:, c0 : c0 + step_cols]).astype(BF16)

            @pl.when(i > 0)
            def _():
                p_copy(i).start()

            return 0

        lax.fori_loop(0, n_tp, one, 0)

    def stage_return():
        flush_slots(packed, landed, d_send, d_recv)
        for i in range(1, n_tp):
            p_arrival(i).wait_recv()
        for j in range(n_lane):
            c = slice(j * LANES, (j + 1) * LANES)
            total = part[tp, :, c].astype(F32)
            for i in range(1, n_tp):
                total = total + precv[up(i), :, c].astype(F32)
            to_tiles(j, total)
        pack_tiles(packed)
        send_slots(packed, returned, e_send, e_recv)

    def step(t, _):
        k = t // 2
        near = lax.rem(t, 2) == 0

        @pl.when(jnp.logical_and(near, k + 1 < depth))
        def _():
            chip = side(k + 1)
            kv_arrival(chip).wait_recv()
            onward(chip).start()
            across(chip, core).start()

        @pl.when(near)
        def _():
            chip = far_side(k)
            kv_arrival(chip).wait_recv()
            across(chip, core).start()

        chip = jnp.where(near, side(k), far_side(k))
        across(chip, 1 - core).wait_recv()
        absorb_chip(chip)

        @pl.when(t == stages[0])
        def _():
            stage_rows()

        @pl.when(t == stages[1])
        def _():
            stage_experts()

        @pl.when(t == stages[2])
        def _():
            stage_return()

        return 0

    lax.fori_loop(0, 2 * depth, step, 0)

    lam = lam_ref[head]
    gain = column(gain_ref[...]) * OUT_SCALE

    def finish(i, _):
        one = acc_ref[2 * i, 0:DV] / acc_ref[2 * i, DV : DV + 1]
        two = acc_ref[2 * i + 1, 0:DV] / acc_ref[2 * i + 1, DV : DV + 1]
        differ = one - lam * two
        scale = lax.rsqrt(jnp.mean(differ * differ, axis=0, keepdims=True) + HEAD_EPS)
        h_out[i] = (differ * scale * gain).astype(BF16)
        return 0

    lax.fori_loop(0, parts, finish, 0)

    def h_copy(i):
        return remote(h_out.at[i], h_in.at[head], h_send.at[i], h_recv.at[head], asks(i))

    def h_arrival(h):
        return remote(h_in.at[h], h_in.at[h], h_send.at[0], h_recv.at[h], attends(h))

    def h_own(i):
        h_in[head] = h_out[i]

    each(parts, asks, lambda i: h_copy(i).start(), h_own)
    weight_copies[3].wait()
    each(heads, attends, lambda h: h_arrival(h).wait_recv(), None)

    head_rows = h_in[...].astype(F32).reshape(heads * DV, rows).T.astype(BF16)
    for c0 in range(0, width, step_cols):
        share = dot(head_rows, ow[:, c0 : c0 + step_cols]).astype(BF16)
        for d in range(n_tp):
            mp[d, :, c0 : c0 + step_cols] = share[tokens * d : tokens * (d + 1)]

    def m_copy(i):
        return tp_copy(mp.at[up(i)], mrecv.at[tp], up(i), m_send.at[i], m_recv.at[i])

    def m_arrival(i):
        here = mrecv.at[down(i)]
        return tp_copy(here, here, down(i), m_send.at[i], m_recv.at[i])

    for i in range(1, n_tp):
        m_copy(i).start()

    take_slots(returned, e_send, e_recv)
    unpack_tiles(returned)
    for j in range(n_lane):
        comb[:, j * LANES : (j + 1) * LANES] = wide[pl.ds(j, slots, stride=n_lane), :].astype(BF16)
    logits = logit_ref[...]
    low, high = logits[0:1], logits[1:2]

    def picked(slot):
        return lax.dot_general(picks(slot), comb[...], (((0,), (0,)), ((), ())), preferred_element_type=F32)

    combined = picked(slot_first) * column(1.0 / (1.0 + jnp.exp(high - low)))
    combined = combined + picked(slot_second) * column(1.0 / (jnp.exp(low - high) + 1.0))
    post = lax.rsqrt(jnp.mean(combined * combined, axis=-1, keepdims=True) + POST_EPS)
    eo_ref[...] = (combined * post).astype(BF16)

    for i in range(1, n_tp):
        m_arrival(i).wait_recv()
    mixed = mp[tp].astype(F32)
    for i in range(1, n_tp):
        mixed = mixed + mrecv[down(i)].astype(F32)
    mix_ref[...] = mixed.astype(BF16)

    flush_slots(packed, returned, e_send, e_recv)
    for i in range(1, n_tp):
        x_copy(i).wait_send()
        p_copy(i).wait_send()
        m_copy(i).wait_send()
    each(heads, attends, lambda h: q_copy(h).wait_send(), None)
    each(parts, asks, lambda i: h_copy(i).wait_send(), None)

    def gone(j, _):
        kv_copy(j).wait_send()
        return 0

    lax.fori_loop(1, heads, gone, 0)

    def forwarded(k, _):
        onward(side(k)).wait_send()
        across(side(k), core).wait_send()
        across(far_side(k), core).wait_send()
        return 0

    lax.fori_loop(0, depth, forwarded, 0)


def local(
    n_ep, n_tp,
    queries, key_rows, value_rows, mix_lambda, head_gain, out_weight, expert_in, expert_gain,
    routes, route_logits, gate_weight, up_weight, down_weight,
):
    rows, cols = queries.shape
    heads = cols // (2 * DQK)
    tokens, width = expert_in.shape
    fe = gate_weight.shape[2]
    top = routes.shape[1]
    cap = (5 * tokens * top + 4 * n_ep - 1) // (4 * n_ep)
    slots = n_ep * cap
    n_lane = width // LANES
    parts = n_ep // 4
    last = n_ep // 2 - 1
    stages = (min(5, last), min(9, last), min(13, last))
    assert n_ep == 4 * heads
    dma = pltpu.SemaphoreType.DMA
    vmem = pl.BlockSpec(memory_space=pltpu.VMEM)
    whole = pl.BlockSpec(memory_space=pl.ANY)
    out = jax.ShapeDtypeStruct((tokens, width), BF16)
    return pl.pallas_call(
        functools.partial(kernel, n_ep, n_tp, cap, stages),
        out_shape=(out, out),
        in_specs=[vmem, vmem, vmem, pl.BlockSpec(memory_space=pltpu.SMEM), vmem, vmem, vmem, vmem, vmem]
        + [whole] * 4,
        out_specs=(vmem, vmem),
        scratch_shapes=[
            pltpu.VMEM((heads, rows, PAIR), BF16),
            pltpu.VMEM((n_ep, rows, PAIR), BF16),
            pltpu.VMEM((heads, 2 * DQK, rows), BF16),
            pltpu.VMEM((parts, 2 * DQK, rows), BF16),
            pltpu.VMEM((2 * parts, PAIR, rows), BF16),
            pltpu.VMEM((DV + ONES, 2 * rows), BF16),
            pltpu.VMEM((2 * parts, 1, rows), F32),
            pltpu.VMEM((2 * parts, DV + ONES, rows), F32),
            pltpu.VMEM((parts, DV, rows), BF16),
            pltpu.VMEM((heads, DV, rows), BF16),
            pltpu.VMEM((width, fe), BF16),
            pltpu.VMEM((width, fe), BF16),
            pltpu.VMEM((fe, width), BF16),
            pltpu.VMEM(out_weight.shape, BF16),
            pltpu.VMEM((slots * n_lane, LANES), F32),
            pltpu.VMEM((slots, n_lane, LANES), BF16),
            pltpu.VMEM((slots, n_lane, LANES), BF16),
            pltpu.VMEM((n_tp, slots, width), BF16),
            pltpu.VMEM((slots, fe), BF16),
            pltpu.VMEM((n_tp, slots, width), BF16),
            pltpu.VMEM((n_tp, slots, width), BF16),
            pltpu.VMEM((slots, n_lane, LANES), BF16),
            pltpu.VMEM((slots, width), BF16),
            pltpu.VMEM((n_tp, tokens, width), BF16),
            pltpu.VMEM((n_tp, tokens, width), BF16),
            dma((4,)),
            dma((n_ep,)), dma((n_ep,)),
            dma((heads,)), dma((parts,)),
            dma((heads,)), dma((n_ep // 2,)), dma((n_ep // 2,)), dma((n_ep // 2,)), dma((n_ep // 2,)),
            dma((parts,)), dma((heads,)),
            dma((n_tp,)), dma((n_tp,)),
            dma((n_tp,)), dma((n_tp,)),
            dma((n_ep,)), dma((n_ep,)),
            dma((n_tp,)), dma((n_tp,)),
        ],
        compiler_params=pltpu.CompilerParams(
            collective_id=0, has_side_effects=True, vmem_limit_bytes=63 * 1024 * 1024
        ),
        name="mixer_and_experts",
    )(
        queries, key_rows, value_rows, mix_lambda, head_gain.reshape(1, DV), expert_in,
        expert_gain.reshape(1, width), routes.T, route_logits.T, out_weight,
        gate_weight[0], up_weight[0], down_weight[0],
    )


def solution(mesh):
    every = ("grp", "ep", "tp")
    return jax.shard_map(
        functools.partial(local, mesh.shape["ep"], mesh.shape["tp"]),
        mesh=mesh,
        in_specs=(
            P(("grp", "ep"), "tp"), P(("grp", "ep"), "tp"), P(("grp", "ep"), "tp"),
            P("tp"), P(), P("tp", None), P(every, None), P(), P(every, None), P(every, None),
            P("ep", None, "tp"), P("ep", None, "tp"), P("ep", "tp", None),
        ),
        out_specs=(P(every, None), P(every, None)),
        check_vma=False,
    )
```

```python
import functools
import math

import jax
import jax.numpy as jnp
from jax import lax
from jax.experimental import pallas as pl
from jax.experimental.pallas import tpu as pltpu
from jax.sharding import PartitionSpec as P

DQK = 32
DV = 64
HEAD_EPS = 0.0001
NORM_EPS = 0.1
POST_EPS = 1.0
CLAMP_LIMIT = 7.0
SIGMOID_SCALE = 1.702
OUT_SCALE = 0.8
CEXP = DQK ** -0.5 * math.log2(math.e)
LANES = 128
PAIR = 2 * DQK + DV
ONES = 16
STAGES = (1, 5, 6, 10)
LOOK = 3
MESH = pl.DeviceIdType.MESH
F32, BF16 = jnp.float32, jnp.bfloat16


def dot(a, b):
    return jnp.dot(a, b, preferred_element_type=F32)


def kernel(
    n_ep, n_tp, cap, stages,
    q_ref, k_ref, v_ref, lam_ref, gain_ref, x_ref, eg_ref, routes_ref, logit_ref,
    ow_hbm, gw_hbm, uw_hbm, dw_hbm,
    mix_ref, eo_ref,
    kv_out, kv_in, q_out, q_in, q_mask, vt_ref, m_ref, acc_ref, h_out, h_in,
    gw, uw, dw, ow,
    wide, packed, landed, xrows, act, part, precv, going, returned, comb, mp, mrecv,
    wsem, d_send, d_recv, q_send, q_recv, k_send, k_recv, f_send, b_send, b_recv, h_send, h_recv,
    x_send, x_recv, p_send, p_recv, e_send, e_recv, m_send, m_recv,
):
    ep, tp = lax.axis_index("ep"), lax.axis_index("tp")
    n_z = n_ep // 2
    depth = n_z // 2
    z, core = ep // 2, lax.rem(ep, 2)
    sibling = 2 * z + 1 - core
    head, odd = z // 2, lax.rem(z, 2)
    partner = z + 1 - 2 * odd
    parts = n_ep // 4
    quarter = ep // parts
    rows = q_ref.shape[0]
    heads = q_ref.shape[1] // (2 * DQK)
    units = 2 * parts
    tokens, width = x_ref.shape
    n_lane = width // LANES
    slots = n_ep * cap
    fe = gw.shape[1]
    band = slots // 2

    weight_copies = [
        pltpu.make_async_copy(src, dst, wsem.at[i])
        for i, (src, dst) in enumerate(((gw_hbm, gw), (uw_hbm, uw), (dw_hbm, dw), (ow_hbm, ow)))
    ]
    for copy in weight_copies:
        copy.start()

    barrier = pltpu.get_barrier_semaphore()

    def greet_ep(d, _):
        pl.semaphore_signal(barrier, inc=1, device_id={"ep": lax.rem(ep + d, n_ep)}, device_id_type=MESH)
        return 0

    def greet_tp(d, _):
        pl.semaphore_signal(barrier, inc=1, device_id={"tp": lax.rem(tp + d, n_tp)}, device_id_type=MESH)
        return 0

    lax.fori_loop(1, n_ep, greet_ep, 0)
    lax.fori_loop(1, n_tp, greet_tp, 0)

    routes = routes_ref[...].astype(F32)
    first, second = routes[0:1], routes[1:2]
    experts = lax.broadcasted_iota(jnp.int32, (n_ep, tokens), 0).astype(F32)
    is_first = (first == experts).astype(F32)
    is_second = (second == experts).astype(F32)
    earlier = (
        lax.broadcasted_iota(jnp.int32, (tokens, tokens), 0)
        < lax.broadcasted_iota(jnp.int32, (tokens, tokens), 1)
    ).astype(BF16)
    ahead = dot((is_first + is_second).astype(BF16), earlier)
    slot_first = first * cap + jnp.sum(ahead * is_first, axis=0, keepdims=True)
    slot_second = second * cap + jnp.sum(ahead * is_second, axis=0, keepdims=True)

    def picks(slot):
        grid = lax.broadcasted_iota(jnp.int32, (slots, tokens), 0).astype(F32)
        return (slot == grid).astype(BF16)

    def column(row):
        n = row.shape[1]
        eye = lax.broadcasted_iota(jnp.int32, (n, n), 0) == lax.broadcasted_iota(jnp.int32, (n, n), 1)
        return jnp.sum(jnp.where(eye, row, 0.0), axis=1, keepdims=True)

    x = x_ref[...].astype(F32)
    normed = x * lax.rsqrt(jnp.mean(x * x, axis=-1, keepdims=True) + NORM_EPS)
    normed = (normed * eg_ref[...]).astype(BF16)
    placing = picks(slot_first) + picks(slot_second)

    def to_tiles(j, columns):
        wide[pl.ds(j, columns.shape[0], stride=n_lane), :] = columns

    step_cols = min(width, 512)
    for c0 in range(0, width, step_cols):
        placed = dot(placing, normed[:, c0 : c0 + step_cols])
        for c1 in range(0, step_cols, LANES):
            to_tiles((c0 + c1) // LANES, placed[:, c1 : c1 + LANES])

    def pack_tiles(dst, base, count):
        def one(i, _):
            block = wide[pl.ds(pl.multiple_of(i * cap * n_lane, n_lane), cap * n_lane), :]
            dst[pl.ds(base + i * cap, cap)] = block.reshape(cap, n_lane, LANES).astype(BF16)
            return 0

        lax.fori_loop(0, count, one, 0)

    def unpack_tiles(src, base, count):
        def one(i, _):
            block = src[pl.ds(base + i * cap, cap)].astype(F32)
            wide[pl.ds(pl.multiple_of(i * cap * n_lane, n_lane), cap * n_lane), :] = block.reshape(cap * n_lane, LANES)
            return 0

        lax.fori_loop(0, count, one, 0)

    pack_tiles(packed, 0, n_ep)

    q_out[...] = q_ref[...].astype(F32).T.reshape(heads, 2 * DQK, rows).astype(BF16)
    for h in range(heads):
        c = slice(DV * h, DV * h + DV)
        kv_out[h] = jnp.concatenate([k_ref[:, c].astype(F32), v_ref[:, c].astype(F32)], axis=1).astype(BF16)
    vt_ref[DV:, :] = jnp.ones((ONES, 2 * rows), BF16)
    for u in range(units):
        m_ref[u] = jnp.full((1, rows), -1e30, F32)
        acc_ref[u] = jnp.zeros((DV + ONES, rows), F32)

    pl.semaphore_wait(barrier, n_ep - 1 + n_tp - 1)

    fourth = n_ep // 4

    def place(d):
        return jnp.where(d <= fourth, d, jnp.where(d > 3 * fourth, d - 2 * fourth, d + fourth - 1))

    def ep_copy(src, dst, send, recv, to):
        return pltpu.make_async_remote_copy(
            src_ref=src, dst_ref=dst, send_sem=send, recv_sem=recv,
            device_id={"ep": to}, device_id_type=MESH,
        )

    def ahead_of(d):
        return lax.rem(ep + d, n_ep)

    def behind(d):
        return lax.rem(ep + n_ep - d, n_ep)

    def out_copy(d):
        to = ahead_of(d)
        return ep_copy(packed.at[pl.ds(to * cap, cap)], landed.at[pl.ds(place(d) * cap, cap)], d_send.at[d], d_recv.at[d], to)

    def out_arrival(d):
        here = landed.at[pl.ds(place(d) * cap, cap)]
        return ep_copy(here, here, d_send.at[d], d_recv.at[d], behind(d))

    def back_copy(d):
        return ep_copy(going.at[pl.ds(place(d) * cap, cap)], returned.at[pl.ds(ep * cap, cap)], e_send.at[d], e_recv.at[d], behind(d))

    def back_arrival(d):
        here = returned.at[pl.ds(ahead_of(d) * cap, cap)]
        return ep_copy(here, here, e_send.at[d], e_recv.at[d], ahead_of(d))

    def over_half(half, act_on):
        def pair(i, _):
            act_on(i)
            act_on(n_ep - i)
            return 0

        if half == 0:
            lax.fori_loop(1, fourth, pair, 0)
            act_on(fourth)
        else:
            act_on(3 * fourth)
            lax.fori_loop(fourth + 1, 2 * fourth, pair, 0)
            act_on(2 * fourth)

    over_half(0, lambda d: out_copy(d).start())
    landed[0:cap] = packed[pl.ds(ep * cap, cap)]

    def remote(src, dst, send, recv, to):
        return pltpu.make_async_remote_copy(
            src_ref=src, dst_ref=dst, send_sem=send, recv_sem=recv,
            device_id={"ep": to}, device_id_type=MESH,
        )

    def each(count, act_on, body, own):
        def one(i, _):
            @pl.when(act_on(i) != ep)
            def _():
                body(i)

            if own is not None:

                @pl.when(act_on(i) == ep)
                def _():
                    own(i)

            return 0

        lax.fori_loop(0, count, one, 0)

    def attends(h):
        return 4 * h + quarter

    def asks(i):
        return parts * lax.rem(ep, 4) + i

    def q_copy(h):
        return remote(q_out.at[h], q_in.at[lax.rem(ep, parts)], q_send.at[h], q_recv.at[lax.rem(ep, parts)], attends(h))

    def q_arrival(i):
        return remote(q_in.at[i], q_in.at[i], q_send.at[0], q_recv.at[i], asks(i))

    def q_own(h):
        q_in[lax.rem(ep, parts)] = q_out[h]

    each(heads, attends, lambda h: q_copy(h).start(), q_own)

    def kv_copy(j):
        pair = lax.rem(head + j, heads)
        rightward = 2 * j - odd < depth
        to = 2 * pair + jnp.where(rightward, 0, 1)
        return remote(kv_out.at[pair], kv_in.at[ep], k_send.at[j], k_recv.at[z], 2 * to + core)

    def side(k):
        return lax.rem(z + n_z + jnp.where(odd == 1, k, -k), n_z)

    def far_side(k):
        return lax.rem(partner + n_z + jnp.where(odd == 1, -k, k), n_z)

    def kv_arrival(chip):
        here = kv_in.at[2 * chip + core]
        return remote(here, here, k_send.at[0], k_recv.at[chip], 2 * partner + core)

    def onward(chip):
        here = kv_in.at[2 * chip + core]
        return remote(here, here, f_send.at[chip], k_recv.at[chip], 2 * partner + core)

    def across(chip, owner):
        here = kv_in.at[2 * chip + owner]
        return remote(here, here, b_send.at[chip], b_recv.at[chip], sibling)

    def kv_band(first, last):
        def both(j, _):
            kv_copy(j).start()
            kv_copy(heads - j).start()
            return 0

        stop = heads // 2
        lax.fori_loop(min(first, stop), min(last, stop), both, 0)
        if first <= stop < last:
            kv_copy(stop).start()

    kv_in[ep] = kv_out[head]
    onward(z).start()
    across(z, core).start()
    kv_band(1, 3)
    over_half(1, lambda d: out_copy(d).start())
    kv_band(3, heads)

    def tp_copy(src, dst, to, send, recv):
        return pltpu.make_async_remote_copy(
            src_ref=src, dst_ref=dst, send_sem=send, recv_sem=recv,
            device_id={"tp": to}, device_id_type=MESH,
        )

    def up(i):
        return lax.rem(tp + i, n_tp)

    def down(i):
        return lax.rem(tp + n_tp - i, n_tp)

    def x_copy(half, i):
        block = xrows.at[half, tp]
        return tp_copy(block, block, up(i), x_send.at[half, i], x_recv.at[half, i])

    def stage_rows(half):
        over_half(half, lambda d: out_arrival(d).wait_recv())
        unpack_tiles(landed, half * band, n_ep // 2)
        for j in range(n_lane):
            xrows[half, tp, :, j * LANES : (j + 1) * LANES] = wide[pl.ds(j, band, stride=n_lane), :].astype(BF16)
        for i in range(1, n_tp):
            x_copy(half, i).start()

    def p_copy(half, i):
        return tp_copy(part.at[half, down(i)], precv.at[half, tp], down(i), p_send.at[half, i], p_recv.at[half, i])

    def stage_experts(half):
        if half == 0:
            for copy in weight_copies[:3]:
                copy.wait()
        for i in range(1, n_tp):
            here = xrows.at[half, down(i)]
            tp_copy(here, here, down(i), x_send.at[half, i], x_recv.at[half, i]).wait_recv()
        x_in = xrows[half].reshape(n_tp * band, width)
        cols = min(fe, 256)
        for c0 in range(0, fe, cols):
            gate = jnp.minimum(dot(x_in, gw[:, c0 : c0 + cols]), CLAMP_LIMIT)
            lift = jnp.clip(dot(x_in, uw[:, c0 : c0 + cols]), -CLAMP_LIMIT, CLAMP_LIMIT)
            act[:, c0 : c0 + cols] = (gate * jax.nn.sigmoid(SIGMOID_SCALE * gate) * (lift + 1.0)).astype(BF16)
        for c0 in range(0, width, cols):
            share = dot(act[...], dw[:, c0 : c0 + cols]).astype(BF16)
            part[half, :, :, c0 : c0 + cols] = share.reshape(n_tp, band, cols)
        for i in range(1, n_tp):
            p_copy(half, i).start()

    def stage_return(half):
        for i in range(1, n_tp):
            here = precv.at[half, up(i)]
            tp_copy(here, here, up(i), p_send.at[half, i], p_recv.at[half, i]).wait_recv()
        for j in range(n_lane):
            c = slice(j * LANES, (j + 1) * LANES)
            total = part[half, tp, :, c].astype(F32)
            for i in range(1, n_tp):
                total = total + precv[half, up(i), :, c].astype(F32)
            to_tiles(j, total)
        pack_tiles(going, half * band, n_ep // 2)
        over_half(half, lambda d: back_copy(d).start())
        if half == 0:
            returned[pl.ds(ep * cap, cap)] = going[0:cap]

    stage_rows(0)

    each(parts, asks, lambda i: q_arrival(i).wait_recv(), None)
    row_map = lax.broadcasted_iota(jnp.int32, (PAIR, rows), 0) // DQK

    def mask_queries(i, _):
        block = jnp.concatenate([q_in[i].astype(F32) * CEXP, jnp.zeros((DV, rows), F32)], axis=0)
        for m in (0, 1):
            kept = jnp.where(row_map == m, block, 0.0)
            high = kept.astype(BF16)
            q_mask[2 * i + m, 0:PAIR] = high
            q_mask[2 * i + m, PAIR:] = (kept - high.astype(F32)).astype(BF16)
        return 0

    lax.fori_loop(0, parts, mask_queries, 0)

    def absorb_chip(chip):
        for b in (0, 1):
            turned = kv_in[2 * chip + b].astype(F32).T
            vt_ref[0:DV, b * rows : (b + 1) * rows] = turned[2 * DQK :].astype(BF16)

        def score(u):
            keys = jnp.concatenate([kv_in[2 * chip + b] for b in (0, 1)], axis=0)
            return dot(jnp.concatenate([keys, keys], axis=1), q_mask[u])

        pending = [score(i) for i in range(min(LOOK, units))]
        for u in range(units):
            if u + LOOK < units:
                pending.append(score(u + LOOK))
            s = pending.pop(0)
            m_old = m_ref[u]
            m_new = jnp.maximum(m_old, jnp.max(s, axis=0, keepdims=True))
            weights = jnp.exp2(s - m_new).astype(BF16)
            shrink = jnp.exp2(m_old - m_new)
            acc_ref[u] = acc_ref[u] * shrink + dot(vt_ref[...], weights)
            m_ref[u] = m_new

    def step(t, _):
        k = t // 2
        near = lax.rem(t, 2) == 0

        @pl.when(jnp.logical_and(near, k + 1 < depth))
        def _():
            chip = side(k + 1)
            kv_arrival(chip).wait_recv()
            onward(chip).start()
            across(chip, core).start()

        @pl.when(near)
        def _():
            chip = far_side(k)
            kv_arrival(chip).wait_recv()
            across(chip, core).start()

        chip = jnp.where(near, side(k), far_side(k))
        across(chip, 1 - core).wait_recv()
        absorb_chip(chip)

        @pl.when(t == stages[0])
        def _():
            stage_experts(0)

        @pl.when(t == stages[1])
        def _():
            stage_return(0)

        @pl.when(t == stages[2])
        def _():
            stage_rows(1)

        @pl.when(t == stages[3])
        def _():
            stage_experts(1)

        return 0

    lax.fori_loop(0, 2 * depth, step, 0)

    lam = lam_ref[head]
    gain = column(gain_ref[...]) * OUT_SCALE

    def finish(i, _):
        one = acc_ref[2 * i, 0:DV] / acc_ref[2 * i, DV : DV + 1]
        two = acc_ref[2 * i + 1, 0:DV] / acc_ref[2 * i + 1, DV : DV + 1]
        differ = one - lam * two
        scale = lax.rsqrt(jnp.mean(differ * differ, axis=0, keepdims=True) + HEAD_EPS)
        h_out[i] = (differ * scale * gain).astype(BF16)
        return 0

    lax.fori_loop(0, parts, finish, 0)

    def h_copy(i):
        return remote(h_out.at[i], h_in.at[head], h_send.at[i], h_recv.at[head], asks(i))

    def h_arrival(h):
        return remote(h_in.at[h], h_in.at[h], h_send.at[0], h_recv.at[h], attends(h))

    def h_own(i):
        h_in[head] = h_out[i]

    each(parts, asks, lambda i: h_copy(i).start(), h_own)
    stage_return(1)
    weight_copies[3].wait()
    each(heads, attends, lambda h: h_arrival(h).wait_recv(), None)

    head_rows = h_in[...].astype(F32).reshape(heads * DV, rows).T.astype(BF16)
    for c0 in range(0, width, step_cols):
        share = dot(head_rows, ow[:, c0 : c0 + step_cols]).astype(BF16)
        for d in range(n_tp):
            mp[d, :, c0 : c0 + step_cols] = share[tokens * d : tokens * (d + 1)]

    def m_copy(i):
        return tp_copy(mp.at[up(i)], mrecv.at[tp], up(i), m_send.at[i], m_recv.at[i])

    def m_arrival(i):
        here = mrecv.at[down(i)]
        return tp_copy(here, here, down(i), m_send.at[i], m_recv.at[i])

    for i in range(1, n_tp):
        m_copy(i).start()

    for half in (0, 1):
        over_half(half, lambda d: back_arrival(d).wait_recv())
    unpack_tiles(returned, 0, n_ep)
    for j in range(n_lane):
        comb[:, j * LANES : (j + 1) * LANES] = wide[pl.ds(j, slots, stride=n_lane), :].astype(BF16)
    logits = logit_ref[...]
    low, high = logits[0:1], logits[1:2]

    def picked(slot):
        return lax.dot_general(picks(slot), comb[...], (((0,), (0,)), ((), ())), preferred_element_type=F32)

    combined = picked(slot_first) * column(1.0 / (1.0 + jnp.exp(high - low)))
    combined = combined + picked(slot_second) * column(1.0 / (jnp.exp(low - high) + 1.0))
    post = lax.rsqrt(jnp.mean(combined * combined, axis=-1, keepdims=True) + POST_EPS)
    eo_ref[...] = (combined * post).astype(BF16)

    for i in range(1, n_tp):
        m_arrival(i).wait_recv()
    mixed = mp[tp].astype(F32)
    for i in range(1, n_tp):
        mixed = mixed + mrecv[down(i)].astype(F32)
    mix_ref[...] = mixed.astype(BF16)

    for half in (0, 1):
        over_half(half, lambda d: out_copy(d).wait_send())
        over_half(half, lambda d: back_copy(d).wait_send())
        for i in range(1, n_tp):
            x_copy(half, i).wait_send()
            p_copy(half, i).wait_send()
    for i in range(1, n_tp):
        m_copy(i).wait_send()
    each(heads, attends, lambda h: q_copy(h).wait_send(), None)
    each(parts, asks, lambda i: h_copy(i).wait_send(), None)

    def gone(j, _):
        kv_copy(j).wait_send()
        return 0

    lax.fori_loop(1, heads, gone, 0)

    def forwarded(k, _):
        onward(side(k)).wait_send()
        across(side(k), core).wait_send()
        across(far_side(k), core).wait_send()
        return 0

    lax.fori_loop(0, depth, forwarded, 0)


def local(
    n_ep, n_tp,
    queries, key_rows, value_rows, mix_lambda, head_gain, out_weight, expert_in, expert_gain,
    routes, route_logits, gate_weight, up_weight, down_weight,
):
    rows, cols = queries.shape
    heads = cols // (2 * DQK)
    tokens, width = expert_in.shape
    fe = gate_weight.shape[2]
    top = routes.shape[1]
    cap = (5 * tokens * top + 4 * n_ep - 1) // (4 * n_ep)
    slots = n_ep * cap
    n_lane = width // LANES
    parts = n_ep // 4
    last = n_ep // 2 - 1
    stages = tuple(min(t, last) for t in STAGES)
    assert n_ep == 4 * heads
    dma = pltpu.SemaphoreType.DMA
    vmem = pl.BlockSpec(memory_space=pltpu.VMEM)
    whole = pl.BlockSpec(memory_space=pl.ANY)
    out = jax.ShapeDtypeStruct((tokens, width), BF16)
    return pl.pallas_call(
        functools.partial(kernel, n_ep, n_tp, cap, stages),
        out_shape=(out, out),
        in_specs=[vmem, vmem, vmem, pl.BlockSpec(memory_space=pltpu.SMEM), vmem, vmem, vmem, vmem, vmem]
        + [whole] * 4,
        out_specs=(vmem, vmem),
        scratch_shapes=[
            pltpu.VMEM((heads, rows, PAIR), BF16),
            pltpu.VMEM((n_ep, rows, PAIR), BF16),
            pltpu.VMEM((heads, 2 * DQK, rows), BF16),
            pltpu.VMEM((parts, 2 * DQK, rows), BF16),
            pltpu.VMEM((2 * parts, 2 * PAIR, rows), BF16),
            pltpu.VMEM((DV + ONES, 2 * rows), BF16),
            pltpu.VMEM((2 * parts, 1, rows), F32),
            pltpu.VMEM((2 * parts, DV + ONES, rows), F32),
            pltpu.VMEM((parts, DV, rows), BF16),
            pltpu.VMEM((heads, DV, rows), BF16),
            pltpu.VMEM((width, fe), BF16),
            pltpu.VMEM((width, fe), BF16),
            pltpu.VMEM((fe, width), BF16),
            pltpu.VMEM(out_weight.shape, BF16),
            pltpu.VMEM((slots * n_lane, LANES), F32),
            pltpu.VMEM((slots, n_lane, LANES), BF16),
            pltpu.VMEM((slots, n_lane, LANES), BF16),
            pltpu.VMEM((2, n_tp, slots // 2, width), BF16),
            pltpu.VMEM((n_tp * slots // 2, fe), BF16),
            pltpu.VMEM((2, n_tp, slots // 2, width), BF16),
            pltpu.VMEM((2, n_tp, slots // 2, width), BF16),
            pltpu.VMEM((slots, n_lane, LANES), BF16),
            pltpu.VMEM((slots, n_lane, LANES), BF16),
            pltpu.VMEM((slots, width), BF16),
            pltpu.VMEM((n_tp, tokens, width), BF16),
            pltpu.VMEM((n_tp, tokens, width), BF16),
            dma((4,)),
            dma((n_ep,)), dma((n_ep,)),
            dma((heads,)), dma((parts,)),
            dma((heads,)), dma((n_ep // 2,)), dma((n_ep // 2,)), dma((n_ep // 2,)), dma((n_ep // 2,)),
            dma((parts,)), dma((heads,)),
            dma((2, n_tp)), dma((2, n_tp)),
            dma((2, n_tp)), dma((2, n_tp)),
            dma((n_ep,)), dma((n_ep,)),
            dma((n_tp,)), dma((n_tp,)),
        ],
        compiler_params=pltpu.CompilerParams(
            collective_id=0, has_side_effects=True, vmem_limit_bytes=63 * 1024 * 1024
        ),
        name="mixer_and_experts",
    )(
        queries, key_rows, value_rows, mix_lambda, head_gain.reshape(1, DV), expert_in,
        expert_gain.reshape(1, width), routes.T, route_logits.T, out_weight,
        gate_weight[0], up_weight[0], down_weight[0],
    )


def solution(mesh):
    every = ("grp", "ep", "tp")
    return jax.shard_map(
        functools.partial(local, mesh.shape["ep"], mesh.shape["tp"]),
        mesh=mesh,
        in_specs=(
            P(("grp", "ep"), "tp"), P(("grp", "ep"), "tp"), P(("grp", "ep"), "tp"),
            P("tp"), P(), P("tp", None), P(every, None), P(), P(every, None), P(every, None),
            P("ep", None, "tp"), P("ep", None, "tp"), P("ep", "tp", None),
        ),
        out_specs=(P(every, None), P(every, None)),
        check_vma=False,
    )
```

```python
import functools
import math

import jax
import jax.numpy as jnp
from jax import lax
from jax.experimental import pallas as pl
from jax.experimental.pallas import tpu as pltpu
from jax.sharding import PartitionSpec as P

DQK = 32
DV = 64
HEAD_EPS = 0.0001
NORM_EPS = 0.1
POST_EPS = 1.0
CLAMP_LIMIT = 7.0
SIGMOID_SCALE = 1.702
OUT_SCALE = 0.8
CEXP = DQK ** -0.5 * math.log2(math.e)
LANES = 128
PAIR = 2 * DQK + DV
ONES = 16
STAGES = (1, 5, 6, 10)
LOOK = 3
MESH = pl.DeviceIdType.MESH
F32, BF16 = jnp.float32, jnp.bfloat16


def dot(a, b):
    return jnp.dot(a, b, preferred_element_type=F32)


def kernel(
    n_ep, n_tp, cap, stages,
    q_ref, k_ref, v_ref, lam_ref, gain_ref, x_ref, eg_ref, routes_ref, logit_ref,
    ow_hbm, gw_hbm, uw_hbm, dw_hbm,
    mix_ref, eo_ref,
    kv_out, kv_in, q_out, q_in, q_mask, vt_ref, m_ref, acc_ref, h_out, h_in,
    gw, uw, dw, ow,
    wide, packed, landed, xrows, act, part, precv, going, returned, comb, mp, mrecv,
    wsem, d_send, d_recv, q_send, q_recv, k_send, k_recv, f_send, b_send, b_recv, h_send, h_recv,
    x_send, x_recv, p_send, p_recv, e_send, e_recv, m_send, m_recv,
):
    ep, tp = lax.axis_index("ep"), lax.axis_index("tp")
    n_z = n_ep // 2
    depth = n_z // 2
    z, core = ep // 2, lax.rem(ep, 2)
    sibling = 2 * z + 1 - core
    head, odd = z // 2, lax.rem(z, 2)
    partner = z + 1 - 2 * odd
    parts = n_ep // 4
    quarter = ep // parts
    rows = q_ref.shape[0]
    heads = q_ref.shape[1] // (2 * DQK)
    units = 2 * parts
    tokens, width = x_ref.shape
    n_lane = width // LANES
    slots = n_ep * cap
    fe = gw.shape[1]
    band = slots // 2

    weight_copies = [
        pltpu.make_async_copy(src, dst, wsem.at[i])
        for i, (src, dst) in enumerate(((gw_hbm, gw), (uw_hbm, uw), (dw_hbm, dw), (ow_hbm, ow)))
    ]
    for copy in weight_copies:
        copy.start()

    barrier = pltpu.get_barrier_semaphore()

    def greet_ep(d, _):
        pl.semaphore_signal(barrier, inc=1, device_id={"ep": lax.rem(ep + d, n_ep)}, device_id_type=MESH)
        return 0

    def greet_tp(d, _):
        pl.semaphore_signal(barrier, inc=1, device_id={"tp": lax.rem(tp + d, n_tp)}, device_id_type=MESH)
        return 0

    lax.fori_loop(1, n_ep, greet_ep, 0)
    lax.fori_loop(1, n_tp, greet_tp, 0)

    routes = routes_ref[...].astype(F32)
    first, second = routes[0:1], routes[1:2]
    experts = lax.broadcasted_iota(jnp.int32, (n_ep, tokens), 0).astype(F32)
    is_first = (first == experts).astype(F32)
    is_second = (second == experts).astype(F32)
    earlier = (
        lax.broadcasted_iota(jnp.int32, (tokens, tokens), 0)
        < lax.broadcasted_iota(jnp.int32, (tokens, tokens), 1)
    ).astype(BF16)
    ahead = dot((is_first + is_second).astype(BF16), earlier)
    slot_first = first * cap + jnp.sum(ahead * is_first, axis=0, keepdims=True)
    slot_second = second * cap + jnp.sum(ahead * is_second, axis=0, keepdims=True)

    def picks(slot):
        grid = lax.broadcasted_iota(jnp.int32, (slots, tokens), 0).astype(F32)
        return (slot == grid).astype(BF16)

    def column(row):
        n = row.shape[1]
        eye = lax.broadcasted_iota(jnp.int32, (n, n), 0) == lax.broadcasted_iota(jnp.int32, (n, n), 1)
        return jnp.sum(jnp.where(eye, row, 0.0), axis=1, keepdims=True)

    x = x_ref[...].astype(F32)
    normed = x * lax.rsqrt(jnp.mean(x * x, axis=-1, keepdims=True) + NORM_EPS)
    normed = (normed * eg_ref[...]).astype(BF16)
    placing = picks(slot_first) + picks(slot_second)

    def to_tiles(j, columns):
        wide[pl.ds(j, columns.shape[0], stride=n_lane), :] = columns

    step_cols = min(width, 512)
    for c0 in range(0, width, step_cols):
        placed = dot(placing, normed[:, c0 : c0 + step_cols])
        for c1 in range(0, step_cols, LANES):
            to_tiles((c0 + c1) // LANES, placed[:, c1 : c1 + LANES])

    def pack_tiles(dst, base, count):
        def one(i, _):
            block = wide[pl.ds(pl.multiple_of(i * cap * n_lane, n_lane), cap * n_lane), :]
            dst[pl.ds(base + i * cap, cap)] = block.reshape(cap, n_lane, LANES).astype(BF16)
            return 0

        lax.fori_loop(0, count, one, 0)

    def unpack_tiles(src, base, count):
        def one(i, _):
            block = src[pl.ds(base + i * cap, cap)].astype(F32)
            wide[pl.ds(pl.multiple_of(i * cap * n_lane, n_lane), cap * n_lane), :] = block.reshape(cap * n_lane, LANES)
            return 0

        lax.fori_loop(0, count, one, 0)

    pack_tiles(packed, 0, n_ep)

    q_out[...] = q_ref[...].astype(F32).T.reshape(heads, 2 * DQK, rows).astype(BF16)
    for h in range(heads):
        c = slice(DV * h, DV * h + DV)
        kv_out[h] = jnp.concatenate([k_ref[:, c].astype(F32), v_ref[:, c].astype(F32)], axis=1).astype(BF16)
    vt_ref[DV:, :] = jnp.ones((ONES, 2 * rows), BF16)
    for u in range(units):
        m_ref[u] = jnp.full((1, rows), -1e30, F32)
        acc_ref[u] = jnp.zeros((DV + ONES, rows), F32)

    pl.semaphore_wait(barrier, n_ep - 1 + n_tp - 1)

    fourth = n_ep // 4

    def place(d):
        return jnp.where(d <= fourth, d, jnp.where(d > 3 * fourth, d - 2 * fourth, d + fourth - 1))

    def ep_copy(src, dst, send, recv, to):
        return pltpu.make_async_remote_copy(
            src_ref=src, dst_ref=dst, send_sem=send, recv_sem=recv,
            device_id={"ep": to}, device_id_type=MESH,
        )

    def ahead_of(d):
        return lax.rem(ep + d, n_ep)

    def behind(d):
        return lax.rem(ep + n_ep - d, n_ep)

    def out_copy(d):
        to = ahead_of(d)
        return ep_copy(packed.at[pl.ds(to * cap, cap)], landed.at[pl.ds(place(d) * cap, cap)], d_send.at[d], d_recv.at[d], to)

    def out_arrival(d):
        here = landed.at[pl.ds(place(d) * cap, cap)]
        return ep_copy(here, here, d_send.at[d], d_recv.at[d], behind(d))

    def back_copy(d):
        return ep_copy(going.at[pl.ds(place(d) * cap, cap)], returned.at[pl.ds(ep * cap, cap)], e_send.at[d], e_recv.at[d], behind(d))

    def back_arrival(d):
        here = returned.at[pl.ds(ahead_of(d) * cap, cap)]
        return ep_copy(here, here, e_send.at[d], e_recv.at[d], ahead_of(d))

    def over_half(half, act_on):
        def pair(i, _):
            act_on(i)
            act_on(n_ep - i)
            return 0

        if half == 0:
            lax.fori_loop(1, fourth, pair, 0)
            act_on(fourth)
        else:
            act_on(3 * fourth)
            lax.fori_loop(fourth + 1, 2 * fourth, pair, 0)
            act_on(2 * fourth)

    over_half(0, lambda d: out_copy(d).start())
    landed[0:cap] = packed[pl.ds(ep * cap, cap)]

    def remote(src, dst, send, recv, to):
        return pltpu.make_async_remote_copy(
            src_ref=src, dst_ref=dst, send_sem=send, recv_sem=recv,
            device_id={"ep": to}, device_id_type=MESH,
        )

    def each(count, act_on, body, own):
        def one(i, _):
            @pl.when(act_on(i) != ep)
            def _():
                body(i)

            if own is not None:

                @pl.when(act_on(i) == ep)
                def _():
                    own(i)

            return 0

        lax.fori_loop(0, count, one, 0)

    def attends(h):
        return 4 * h + quarter

    def asks(i):
        return parts * lax.rem(ep, 4) + i

    def q_copy(h):
        return remote(q_out.at[h], q_in.at[lax.rem(ep, parts)], q_send.at[h], q_recv.at[lax.rem(ep, parts)], attends(h))

    def q_arrival(i):
        return remote(q_in.at[i], q_in.at[i], q_send.at[0], q_recv.at[i], asks(i))

    def q_own(h):
        q_in[lax.rem(ep, parts)] = q_out[h]

    each(heads, attends, lambda h: q_copy(h).start(), q_own)

    def kv_copy(j):
        pair = lax.rem(head + j, heads)
        rightward = 2 * j - odd < depth
        to = 2 * pair + jnp.where(rightward, 0, 1)
        return remote(kv_out.at[pair], kv_in.at[ep], k_send.at[j], k_recv.at[z], 2 * to + core)

    def side(k):
        return lax.rem(z + n_z + jnp.where(odd == 1, k, -k), n_z)

    def far_side(k):
        return lax.rem(partner + n_z + jnp.where(odd == 1, -k, k), n_z)

    def kv_arrival(chip):
        here = kv_in.at[2 * chip + core]
        return remote(here, here, k_send.at[0], k_recv.at[chip], 2 * partner + core)

    def onward(chip):
        here = kv_in.at[2 * chip + core]
        return remote(here, here, f_send.at[chip], k_recv.at[chip], 2 * partner + core)

    def across(chip, owner):
        here = kv_in.at[2 * chip + owner]
        return remote(here, here, b_send.at[chip], b_recv.at[chip], sibling)

    def kv_band(first, last):
        def both(j, _):
            kv_copy(j).start()
            kv_copy(heads - j).start()
            return 0

        stop = heads // 2
        lax.fori_loop(min(first, stop), min(last, stop), both, 0)
        if first <= stop < last:
            kv_copy(stop).start()

    kv_in[ep] = kv_out[head]
    onward(z).start()
    across(z, core).start()
    kv_band(1, 3)
    over_half(1, lambda d: out_copy(d).start())
    kv_band(3, heads)

    def tp_copy(src, dst, to, send, recv):
        return pltpu.make_async_remote_copy(
            src_ref=src, dst_ref=dst, send_sem=send, recv_sem=recv,
            device_id={"tp": to}, device_id_type=MESH,
        )

    def up(i):
        return lax.rem(tp + i, n_tp)

    def down(i):
        return lax.rem(tp + n_tp - i, n_tp)

    far_first = sorted(range(1, n_tp), key=lambda i: -min(i, n_tp - i))

    def x_copy(half, i):
        block = xrows.at[half, tp]
        return tp_copy(block, block, up(i), x_send.at[half, i], x_recv.at[half, i])

    def stage_rows(half):
        over_half(half, lambda d: out_arrival(d).wait_recv())
        unpack_tiles(landed, half * band, n_ep // 2)
        for j in range(n_lane):
            xrows[half, tp, :, j * LANES : (j + 1) * LANES] = wide[pl.ds(j, band, stride=n_lane), :].astype(BF16)
        for i in far_first:
            x_copy(half, i).start()

    def p_copy(half, i):
        return tp_copy(part.at[half, down(i)], precv.at[half, tp], down(i), p_send.at[half, i], p_recv.at[half, i])

    def stage_experts(half):
        if half == 0:
            for copy in weight_copies[:3]:
                copy.wait()
        for i in range(1, n_tp):
            here = xrows.at[half, down(i)]
            tp_copy(here, here, down(i), x_send.at[half, i], x_recv.at[half, i]).wait_recv()
        x_in = xrows[half].reshape(n_tp * band, width)
        cols = min(fe, 256)
        for c0 in range(0, fe, cols):
            gate = jnp.minimum(dot(x_in, gw[:, c0 : c0 + cols]), CLAMP_LIMIT)
            lift = jnp.clip(dot(x_in, uw[:, c0 : c0 + cols]), -CLAMP_LIMIT, CLAMP_LIMIT)
            act[:, c0 : c0 + cols] = (gate * jax.nn.sigmoid(SIGMOID_SCALE * gate) * (lift + 1.0)).astype(BF16)
        for c0 in range(0, width, cols):
            share = dot(act[...], dw[:, c0 : c0 + cols]).astype(BF16)
            part[half, :, :, c0 : c0 + cols] = share.reshape(n_tp, band, cols)
        for i in far_first:
            p_copy(half, i).start()

    def stage_return(half):
        for i in range(1, n_tp):
            here = precv.at[half, up(i)]
            tp_copy(here, here, up(i), p_send.at[half, i], p_recv.at[half, i]).wait_recv()
        for j in range(n_lane):
            c = slice(j * LANES, (j + 1) * LANES)
            total = part[half, tp, :, c].astype(F32)
            for i in range(1, n_tp):
                total = total + precv[half, up(i), :, c].astype(F32)
            to_tiles(j, total)
        pack_tiles(going, half * band, n_ep // 2)
        over_half(half, lambda d: back_copy(d).start())
        if half == 0:
            returned[pl.ds(ep * cap, cap)] = going[0:cap]

    stage_rows(0)

    each(parts, asks, lambda i: q_arrival(i).wait_recv(), None)
    row_map = lax.broadcasted_iota(jnp.int32, (PAIR, rows), 0) // DQK

    def mask_queries(i, _):
        block = jnp.concatenate([q_in[i].astype(F32) * CEXP, jnp.zeros((DV, rows), F32)], axis=0)
        for m in (0, 1):
            kept = jnp.where(row_map == m, block, 0.0)
            high = kept.astype(BF16)
            q_mask[2 * i + m, 0:PAIR] = high
            q_mask[2 * i + m, PAIR:] = (kept - high.astype(F32)).astype(BF16)
        return 0

    lax.fori_loop(0, parts, mask_queries, 0)

    def absorb_chip(chip):
        for b in (0, 1):
            turned = kv_in[2 * chip + b].astype(F32).T
            vt_ref[0:DV, b * rows : (b + 1) * rows] = turned[2 * DQK :].astype(BF16)

        def score(u):
            keys = jnp.concatenate([kv_in[2 * chip + b] for b in (0, 1)], axis=0)
            return dot(jnp.concatenate([keys, keys], axis=1), q_mask[u])

        pending = [score(i) for i in range(min(LOOK, units))]
        for u in range(units):
            if u + LOOK < units:
                pending.append(score(u + LOOK))
            s = pending.pop(0)
            m_old = m_ref[u]
            m_new = jnp.maximum(m_old, jnp.max(s, axis=0, keepdims=True))
            weights = jnp.exp2(s - m_new).astype(BF16)
            shrink = jnp.exp2(m_old - m_new)
            acc_ref[u] = acc_ref[u] * shrink + dot(vt_ref[...], weights)
            m_ref[u] = m_new

    def step(t, _):
        k = t // 2
        near = lax.rem(t, 2) == 0

        @pl.when(jnp.logical_and(near, k + 1 < depth))
        def _():
            chip = side(k + 1)
            kv_arrival(chip).wait_recv()
            onward(chip).start()
            across(chip, core).start()

        @pl.when(near)
        def _():
            chip = far_side(k)
            kv_arrival(chip).wait_recv()
            across(chip, core).start()

        chip = jnp.where(near, side(k), far_side(k))
        across(chip, 1 - core).wait_recv()
        absorb_chip(chip)

        @pl.when(t == stages[0])
        def _():
            stage_experts(0)

        @pl.when(t == stages[1])
        def _():
            stage_return(0)

        @pl.when(t == stages[2])
        def _():
            stage_rows(1)

        @pl.when(t == stages[3])
        def _():
            stage_experts(1)

        return 0

    lax.fori_loop(0, 2 * depth, step, 0)

    lam = lam_ref[head]
    gain = column(gain_ref[...]) * OUT_SCALE

    def finish(i, _):
        one = acc_ref[2 * i, 0:DV] / acc_ref[2 * i, DV : DV + 1]
        two = acc_ref[2 * i + 1, 0:DV] / acc_ref[2 * i + 1, DV : DV + 1]
        differ = one - lam * two
        scale = lax.rsqrt(jnp.mean(differ * differ, axis=0, keepdims=True) + HEAD_EPS)
        h_out[i] = (differ * scale * gain).astype(BF16)
        return 0

    lax.fori_loop(0, parts, finish, 0)

    def h_copy(i):
        return remote(h_out.at[i], h_in.at[head], h_send.at[i], h_recv.at[head], asks(i))

    def h_arrival(h):
        return remote(h_in.at[h], h_in.at[h], h_send.at[0], h_recv.at[h], attends(h))

    def h_own(i):
        h_in[head] = h_out[i]

    each(parts, asks, lambda i: h_copy(i).start(), h_own)
    stage_return(1)
    weight_copies[3].wait()
    each(heads, attends, lambda h: h_arrival(h).wait_recv(), None)

    head_rows = h_in[...].astype(F32).reshape(heads * DV, rows).T.astype(BF16)
    side_cols = width // 2
    block_cols = min(side_cols, 512)

    def m_copy(i, c):
        cut = pl.ds(c * side_cols, side_cols)
        return tp_copy(mp.at[up(i), :, cut], mrecv.at[tp, :, cut], up(i), m_send.at[c, i], m_recv.at[c, i])

    def m_arrival(i, c):
        here = mrecv.at[down(i), :, pl.ds(c * side_cols, side_cols)]
        return tp_copy(here, here, down(i), m_send.at[c, i], m_recv.at[c, i])

    for c in (0, 1):
        for c0 in range(c * side_cols, (c + 1) * side_cols, block_cols):
            share = dot(head_rows, ow[:, c0 : c0 + block_cols]).astype(BF16)
            for d in range(n_tp):
                mp[d, :, c0 : c0 + block_cols] = share[tokens * d : tokens * (d + 1)]
        for i in far_first:
            m_copy(i, c).start()

    for half in (0, 1):
        over_half(half, lambda d: back_arrival(d).wait_recv())
    unpack_tiles(returned, 0, n_ep)
    for j in range(n_lane):
        comb[:, j * LANES : (j + 1) * LANES] = wide[pl.ds(j, slots, stride=n_lane), :].astype(BF16)
    logits = logit_ref[...]
    low, high = logits[0:1], logits[1:2]

    def picked(slot):
        return lax.dot_general(picks(slot), comb[...], (((0,), (0,)), ((), ())), preferred_element_type=F32)

    combined = picked(slot_first) * column(1.0 / (1.0 + jnp.exp(high - low)))
    combined = combined + picked(slot_second) * column(1.0 / (jnp.exp(low - high) + 1.0))
    post = lax.rsqrt(jnp.mean(combined * combined, axis=-1, keepdims=True) + POST_EPS)
    eo_ref[...] = (combined * post).astype(BF16)

    for c in (0, 1):
        cut = slice(c * side_cols, (c + 1) * side_cols)
        for i in range(1, n_tp):
            m_arrival(i, c).wait_recv()
        mixed = mp[tp, :, cut].astype(F32)
        for i in range(1, n_tp):
            mixed = mixed + mrecv[down(i), :, cut].astype(F32)
        mix_ref[:, cut] = mixed.astype(BF16)

    for half in (0, 1):
        over_half(half, lambda d: out_copy(d).wait_send())
        over_half(half, lambda d: back_copy(d).wait_send())
        for i in range(1, n_tp):
            x_copy(half, i).wait_send()
            p_copy(half, i).wait_send()
    for i in range(1, n_tp):
        for c in (0, 1):
            m_copy(i, c).wait_send()
    each(heads, attends, lambda h: q_copy(h).wait_send(), None)
    each(parts, asks, lambda i: h_copy(i).wait_send(), None)

    def gone(j, _):
        kv_copy(j).wait_send()
        return 0

    lax.fori_loop(1, heads, gone, 0)

    def forwarded(k, _):
        onward(side(k)).wait_send()
        across(side(k), core).wait_send()
        across(far_side(k), core).wait_send()
        return 0

    lax.fori_loop(0, depth, forwarded, 0)


def local(
    n_ep, n_tp,
    queries, key_rows, value_rows, mix_lambda, head_gain, out_weight, expert_in, expert_gain,
    routes, route_logits, gate_weight, up_weight, down_weight,
):
    rows, cols = queries.shape
    heads = cols // (2 * DQK)
    tokens, width = expert_in.shape
    fe = gate_weight.shape[2]
    top = routes.shape[1]
    cap = (5 * tokens * top + 4 * n_ep - 1) // (4 * n_ep)
    slots = n_ep * cap
    n_lane = width // LANES
    parts = n_ep // 4
    last = n_ep // 2 - 1
    stages = tuple(min(t, last) for t in STAGES)
    assert n_ep == 4 * heads
    dma = pltpu.SemaphoreType.DMA
    vmem = pl.BlockSpec(memory_space=pltpu.VMEM)
    whole = pl.BlockSpec(memory_space=pl.ANY)
    out = jax.ShapeDtypeStruct((tokens, width), BF16)
    return pl.pallas_call(
        functools.partial(kernel, n_ep, n_tp, cap, stages),
        out_shape=(out, out),
        in_specs=[vmem, vmem, vmem, pl.BlockSpec(memory_space=pltpu.SMEM), vmem, vmem, vmem, vmem, vmem]
        + [whole] * 4,
        out_specs=(vmem, vmem),
        scratch_shapes=[
            pltpu.VMEM((heads, rows, PAIR), BF16),
            pltpu.VMEM((n_ep, rows, PAIR), BF16),
            pltpu.VMEM((heads, 2 * DQK, rows), BF16),
            pltpu.VMEM((parts, 2 * DQK, rows), BF16),
            pltpu.VMEM((2 * parts, 2 * PAIR, rows), BF16),
            pltpu.VMEM((DV + ONES, 2 * rows), BF16),
            pltpu.VMEM((2 * parts, 1, rows), F32),
            pltpu.VMEM((2 * parts, DV + ONES, rows), F32),
            pltpu.VMEM((parts, DV, rows), BF16),
            pltpu.VMEM((heads, DV, rows), BF16),
            pltpu.VMEM((width, fe), BF16),
            pltpu.VMEM((width, fe), BF16),
            pltpu.VMEM((fe, width), BF16),
            pltpu.VMEM(out_weight.shape, BF16),
            pltpu.VMEM((slots * n_lane, LANES), F32),
            pltpu.VMEM((slots, n_lane, LANES), BF16),
            pltpu.VMEM((slots, n_lane, LANES), BF16),
            pltpu.VMEM((2, n_tp, slots // 2, width), BF16),
            pltpu.VMEM((n_tp * slots // 2, fe), BF16),
            pltpu.VMEM((2, n_tp, slots // 2, width), BF16),
            pltpu.VMEM((2, n_tp, slots // 2, width), BF16),
            pltpu.VMEM((slots, n_lane, LANES), BF16),
            pltpu.VMEM((slots, n_lane, LANES), BF16),
            pltpu.VMEM((slots, width), BF16),
            pltpu.VMEM((n_tp, tokens, width), BF16),
            pltpu.VMEM((n_tp, tokens, width), BF16),
            dma((4,)),
            dma((n_ep,)), dma((n_ep,)),
            dma((heads,)), dma((parts,)),
            dma((heads,)), dma((n_ep // 2,)), dma((n_ep // 2,)), dma((n_ep // 2,)), dma((n_ep // 2,)),
            dma((parts,)), dma((heads,)),
            dma((2, n_tp)), dma((2, n_tp)),
            dma((2, n_tp)), dma((2, n_tp)),
            dma((n_ep,)), dma((n_ep,)),
            dma((2, n_tp)), dma((2, n_tp)),
        ],
        compiler_params=pltpu.CompilerParams(
            collective_id=0, has_side_effects=True, vmem_limit_bytes=63 * 1024 * 1024
        ),
        name="mixer_and_experts",
    )(
        queries, key_rows, value_rows, mix_lambda, head_gain.reshape(1, DV), expert_in,
        expert_gain.reshape(1, width), routes.T, route_logits.T, out_weight,
        gate_weight[0], up_weight[0], down_weight[0],
    )


def solution(mesh):
    every = ("grp", "ep", "tp")
    return jax.shard_map(
        functools.partial(local, mesh.shape["ep"], mesh.shape["tp"]),
        mesh=mesh,
        in_specs=(
            P(("grp", "ep"), "tp"), P(("grp", "ep"), "tp"), P(("grp", "ep"), "tp"),
            P("tp"), P(), P("tp", None), P(every, None), P(), P(every, None), P(every, None),
            P("ep", None, "tp"), P("ep", None, "tp"), P("ep", "tp", None),
        ),
        out_specs=(P(every, None), P(every, None)),
        check_vma=False,
    )
```
